256 devices in a mesh: ep: 128 (over z, y, x), tp: 2 (over core).
Axes of the slice: x: 4, y: 4, z: 8, core: 2. Of those that a mesh axis runs over, the one named last changes fastest.
Arguments:
- tokens: bfloat16 [2048, 1536], P('ep'), may hold values from -6 to 6
- prior_state: float32 [2048, 12, 64, 64], P('ep', 'tp'), may hold values from -12 to 12
- first_gain: float32 [1536], replicated, may hold values from 0.1 to 1.9
- query_weight: bfloat16 [1536, 768], P(None, 'tp'), may hold values from -0.15625 to 0.15625
- key_weight: bfloat16 [1536, 768], P(None, 'tp'), may hold values from -0.15625 to 0.15625
- value_weight: bfloat16 [1536, 768], P(None, 'tp'), may hold values from -0.15625 to 0.15625
- decay_down: bfloat16 [1536, 96], replicated, may hold values from -0.15625 to 0.15625
- decay_up: bfloat16 [96, 768], P(None, 'tp'), may hold values from -1.25 to 1.25
- decay_base: float32 [768], P('tp'), may hold values from -5 to 1
- rate_down: bfloat16 [1536, 96], replicated, may hold values from -0.15625 to 0.15625
- rate_up: bfloat16 [96, 768], P(None, 'tp'), may hold values from -1.25 to 1.25
- rate_base: float32 [768], P('tp'), may hold values from -4 to 4
- head_gain: float32 [768], P('tp'), may hold values from 0.1 to 1.9
- out_weight: bfloat16 [768, 1536], P('tp'), may hold values from -0.21875 to 0.21875
- mid_gain: float32 [1536], replicated, may hold values from 0.1 to 1.9
- route_ids: int32 [2048, 6], P('ep'), may hold values from 0 to 127, all different within a row; in each aligned block of 16 rows (0 to 15, 16 to 31, ...) at most 2 rows name the same one
- route_weights: float32 [2048, 6], P('ep'), may hold values from 0.1 to 1
- expert_gate: bfloat16 [128, 1536, 384], P('ep', None, 'tp'), may hold values from -0.15625 to 0.15625
- expert_up: bfloat16 [128, 1536, 384], P('ep', None, 'tp'), may hold values from -0.15625 to 0.15625
- expert_down: bfloat16 [128, 384, 1536], P('ep', 'tp'), may hold values from -0.3125 to 0.3125
- dense_gate: bfloat16 [1536, 6144], P(None, ('ep', 'tp')), may hold values from -0.15625 to 0.15625
- dense_up: bfloat16 [1536, 6144], P(None, ('ep', 'tp')), may hold values from -0.15625 to 0.15625
- dense_down: bfloat16 [6144, 1536], P(('ep', 'tp')), may hold values from -0.078125 to 0.078125
- blend_vector: bfloat16 [1536], replicated, may hold values from -0.15625 to 0.15625
Outputs:
- mixed: bfloat16 [2048, 1536], P('ep', 'tp')
- new_state: float32 [2048, 12, 64, 64], P('ep', 'tp')
The draws below stay inside these ranges and needn't reach their ends.
Inputs may be any that keep to these rules, and one draw needn't show every extreme that they name: `route_ids`: each row names 6 different experts; among the rows of one device no expert is named by more than 2 rows, a bound that some block reaches.
All inputs are finite; a program needn't handle non-finite values.
Results may differ from the reference program's by a relative error of at most 0.02.
Values may be sent and summed in bfloat16 or wider, within the bound.
A program may use at most 128 MiB of HBM per device.

```python
import math
import jax
import jax.numpy as jnp
import numpy as np
from jax import lax

D = 1536
HEADS = 12
HEAD = 64
INNER = 768
RANK = 96
FE = 384
FD = 6144
TOP = 6
SEQS = 16
EXPERTS = 128
BATCH = 2048
CAP = 2
N_EP = 128
N_TP = 2


def levels(key, extent, pieces, least, largest):
    level = 1.0
    for axis_at, parts in pieces:
        draws = jax.random.uniform(jax.random.fold_in(jax.random.fold_in(key, 6), axis_at), (parts,), jnp.float32, least / len(pieces), largest / len(pieces))
        level = level * jnp.repeat(jnp.exp(draws), extent[axis_at] // parts).reshape((-1,) + (1,) * (len(extent) - 1 - axis_at))
    return level


def shared_out(rng, own, number, rows, count, top, bound, slope):
    sequence = jax.random.permutation(rng, count)
    crowded, common = shares(count, rows * top, bound, slope, True), shares(count, rows * top, bound, slope, False)
    places = jnp.arange(count)

    def named(tallies, offset_by):
        used = int((tallies > 0).sum())
        fixed = max(1, used // 4)
        passed = fixed + (places - fixed + offset_by * (used - fixed)) % max(1, count - fixed)
        return jnp.zeros((count,), jnp.int32).at[sequence[jnp.where(places < fixed, places, passed)]].set(jnp.asarray(tallies, jnp.int32))

    tallies = jnp.where(number % 4 == 0, named(crowded, number // 4), named(common, number - number // 4 - 1))
    mixed = jax.random.permutation(jax.random.fold_in(own, 3), count)
    donor, taker = mixed[0:count // 2 * 2:2], mixed[1:count // 2 * 2:2]
    room = jnp.minimum(tallies[donor] - 1, bound - tallies[taker]) // 2
    room = jnp.where((donor == sequence[0]) | (taker == sequence[0]) | (tallies[taker] == 0), 0, jnp.maximum(room, 0))
    passed = jax.random.randint(jax.random.fold_in(own, 4), (count // 2,), 0, 1 << 20) % (room + 1)
    tallies = tallies.at[donor].add(-passed).at[taker].add(passed)
    items = jnp.searchsorted(jnp.cumsum(tallies), jnp.arange(rows * top), side="right").astype(jnp.int32)
    table = items.reshape(top, rows).T
    table = table[jax.random.permutation(jax.random.fold_in(own, 1), rows)]
    offset_by = jax.random.randint(jax.random.fold_in(own, 2), (rows, 1), 0, top)
    return jnp.take_along_axis(table, (jnp.arange(top)[None, :] + offset_by) % top, axis=1)


def shares(amount, total, limit, skew, full):
    portions = [(1 << 20) // math.isqrt(standing ** skew) + 1 for standing in range(1, amount + 1)]
    largest = limit if full else min(limit, max(-(-total // amount), total * portions[0] // sum(portions)))
    least = 1 if total - largest >= amount - 1 else 0
    holding, spare = [largest] + [least] * (amount - 1), total - largest - least * (amount - 1)
    while spare > 0:
        free = [i for i in range(1, amount) if holding[i] < largest] or [i for i in range(1, amount) if holding[i] < limit]
        whole, left = sum([portions[i] for i in free]), spare
        for i in free:
            extra = min(limit - holding[i], max(1, left * portions[i] // whole), spare)
            holding[i] = holding[i] + extra
            spare = spare - extra
    return np.array(holding)


def gaussian(stream_key, shape, width, limit, split=(), kind=jnp.bfloat16):
    result = jax.random.normal(stream_key, shape, jnp.float32) * width
    if len(split) > 0:
        result = levels(stream_key, shape, split, -0.22, 0.18) * result
    return jnp.clip(result, min=-limit, max=limit).astype(kind)


def setup_inputs(seed: int = 0) -> dict:
    key_list = jax.random.split(jax.random.key(seed), 25)
    tokens = gaussian(key_list[0], (BATCH, D), 1.0, 6.0, ((0, 128),))
    prior_state = gaussian(key_list[1], (BATCH, HEADS, HEAD, HEAD), 2.0, 12.0, ((0, 128), (1, 2)), jnp.float32)
    first_gain = jnp.clip(1.0 + 0.18 * jax.random.normal(key_list[2], (D,), jnp.float32), 0.1, 1.9)
    query_weight = gaussian(key_list[3], (D, INNER), D ** -0.5, 0.15625, ((1, 2),))
    key_weight = gaussian(key_list[4], (D, INNER), D ** -0.5, 0.15625, ((1, 2),))
    value_weight = gaussian(key_list[5], (D, INNER), D ** -0.5, 0.15625, ((1, 2),))
    decay_down = gaussian(key_list[6], (D, RANK), D ** -0.5, 0.15625)
    decay_up = gaussian(key_list[7], (RANK, INNER), (RANK // 4) ** -0.5, 1.25, ((1, 2),))
    decay_base = jnp.clip(-5.0 + 6.0 * jax.random.uniform(key_list[8], (INNER,), jnp.float32) ** levels(key_list[8], (INNER,), ((0, 2),), -0.2, 0.2), -5.0, 1.0)
    rate_down = gaussian(key_list[9], (D, RANK), D ** -0.5, 0.15625)
    rate_up = gaussian(key_list[10], (RANK, INNER), (RANK // 4) ** -0.5, 1.25, ((1, 2),))
    rate_base = jnp.clip(jax.random.uniform(key_list[11], (INNER,), jnp.float32, -4.0, 4.0) * levels(key_list[11], (INNER,), ((0, 2),), -0.4, 0.0), -4.0, 4.0)
    head_gain = jnp.clip(1.0 + 0.18 * jax.random.normal(key_list[12], (INNER,), jnp.float32), 0.1, 1.9)
    out_weight = gaussian(key_list[13], (INNER, D), INNER ** -0.5, 0.21875, ((0, 2),))
    mid_gain = jnp.clip(1.0 + 0.18 * jax.random.normal(key_list[14], (D,), jnp.float32), 0.1, 1.9)
    route_ids_keys = jax.random.split(jax.random.fold_in(key_list[15], 1), BATCH // SEQS)
    route_ids_turns = jax.random.permutation(jax.random.fold_in(key_list[15], 3), BATCH // SEQS)
    route_ids = jax.vmap(lambda own, number: shared_out(jax.random.fold_in(key_list[15], 2), own, number, SEQS, EXPERTS, TOP, CAP, 2))(route_ids_keys, route_ids_turns).reshape((BATCH, TOP))
    route_weights = jnp.clip(jnp.exp(math.log(1.0) - 2.3025851 * jax.random.uniform(key_list[16], (BATCH, TOP), jnp.float32) ** levels(key_list[16], (BATCH, TOP), ((0, 128),), -0.2, 0.2)), 0.1, 1.0)
    expert_gate = gaussian(key_list[17], (EXPERTS, D, FE), D ** -0.5, 0.15625, ((0, 128), (2, 2)))
    expert_up = gaussian(key_list[18], (EXPERTS, D, FE), D ** -0.5, 0.15625, ((0, 128), (2, 2)))
    expert_down = gaussian(key_list[19], (EXPERTS, FE, D), FE ** -0.5, 0.3125, ((0, 128), (1, 2)))
    dense_gate = gaussian(key_list[20], (D, FD), D ** -0.5, 0.15625, ((1, 256),))
    dense_up = gaussian(key_list[21], (D, FD), D ** -0.5, 0.15625, ((1, 256),))
    dense_down = gaussian(key_list[22], (FD, D), FD ** -0.5, 0.078125, ((0, 256),))
    blend_vector = gaussian(key_list[23], (D,), D ** -0.5, 0.15625)
    return dict(tokens=tokens, prior_state=prior_state, first_gain=first_gain, query_weight=query_weight, key_weight=key_weight, value_weight=value_weight, decay_down=decay_down, decay_up=decay_up, decay_base=decay_base, rate_down=rate_down, rate_up=rate_up, rate_base=rate_base, head_gain=head_gain, out_weight=out_weight, mid_gain=mid_gain, route_ids=route_ids, route_weights=route_weights, expert_gate=expert_gate, expert_up=expert_up, expert_down=expert_down, dense_gate=dense_gate, dense_up=dense_up, dense_down=dense_down, blend_vector=blend_vector)


def rms_norm(values, gain):
    scale = lax.rsqrt(lax.optimization_barrier(jnp.mean(values * values, axis=-1, keepdims=True)) + 1e-06)
    return values * scale * gain.astype(jnp.float32)

def rounded(values):
    return lax.optimization_barrier(values.astype(jnp.bfloat16)).astype(jnp.float32)

def mixer_core(normed, prior_state, query_weight, key_weight, value_weight, decay_down, decay_up, decay_base, rate_down, rate_up, rate_base, head_gain):
    rows = normed.shape[0]
    heads_here = prior_state.shape[1]
    head_size = prior_state.shape[2]

    def project(weight):
        product = jnp.dot(normed, weight, preferred_element_type=jnp.float32)
        return rounded(product).reshape(rows, heads_here, head_size)
    receptance = project(query_weight)
    key_vec = project(key_weight)
    value_vec = project(value_weight)
    decay_low = jnp.tanh(jnp.dot(normed, decay_down, preferred_element_type=jnp.float32)).astype(jnp.bfloat16)
    decay_log = decay_base + jnp.dot(decay_low, decay_up, preferred_element_type=jnp.float32)
    decay_log = -jax.nn.softplus(-decay_log) - 0.5
    decay_rate = jnp.exp(-jnp.exp(decay_log)).reshape(rows, heads_here, head_size)
    rate_low = jnp.dot(normed, rate_down, preferred_element_type=jnp.float32).astype(jnp.bfloat16)
    learn_rate = jax.nn.sigmoid(rate_base + jnp.dot(rate_low, rate_up, preferred_element_type=jnp.float32))
    learn_rate = learn_rate.reshape(rows, heads_here, head_size)
    unit_key = key_vec * lax.rsqrt(lax.optimization_barrier(jnp.sum(key_vec * key_vec, axis=-1, keepdims=True)) + 1e-06)
    removed = lax.optimization_barrier(jnp.sum(prior_state * unit_key[:, :, None, :], axis=-1))
    new_state = prior_state * decay_rate[:, :, None, :] - removed[..., None] * (unit_key * learn_rate)[:, :, None, :] + value_vec[..., None] * key_vec[:, :, None, :]
    read = lax.optimization_barrier(jnp.sum(new_state * receptance[:, :, None, :], axis=-1))
    center = lax.optimization_barrier(jnp.mean(read, axis=-1, keepdims=True))
    spread = lax.optimization_barrier(jnp.mean(jnp.square(read - center), axis=-1, keepdims=True))
    normal = (read - center) * lax.rsqrt(spread + 0.00064)
    mixed_heads = (normal.reshape(rows, -1) * head_gain.astype(jnp.float32)).astype(jnp.bfloat16)
    return (mixed_heads, new_state)

def reference(tokens, prior_state, first_gain, query_weight, key_weight, value_weight, decay_down, decay_up, decay_base, rate_down, rate_up, rate_base, head_gain, out_weight, mid_gain, route_ids, route_weights, expert_gate, expert_up, expert_down, dense_gate, dense_up, dense_down, blend_vector):
    token_f = tokens.astype(jnp.float32)
    normed = rms_norm(token_f, first_gain).astype(jnp.bfloat16)
    mixed_heads, new_state = mixer_core(normed, prior_state, query_weight, key_weight, value_weight, decay_down, decay_up, decay_base, rate_down, rate_up, rate_base, head_gain)
    block = INNER // N_TP
    attn = jnp.zeros((BATCH, D), jnp.float32)
    for part_idx in range(N_TP):
        lower = part_idx * block
        attn = attn + rounded(jnp.dot(mixed_heads[:, lower:lower + block], out_weight[lower:lower + block], preferred_element_type=jnp.float32))
    resid = rounded(token_f + attn)
    mid = rms_norm(resid, mid_gain).astype(jnp.bfloat16)
    blend = jax.nn.sigmoid(jnp.dot(mid, blend_vector, preferred_element_type=jnp.float32))
    flat_ids = route_ids.reshape(N_EP, SEQS * TOP)
    onehot = (flat_ids[..., None] == jnp.arange(EXPERTS, dtype=jnp.int32)[None, None, :]).astype(jnp.int32)
    before = jnp.cumsum(onehot, axis=1) - onehot
    position = lax.optimization_barrier(jnp.sum(onehot * before, axis=-1))
    group_ids = jnp.arange(N_EP, dtype=jnp.int32)[:, None]
    slot = (flat_ids * (N_EP * CAP) + group_ids * CAP + position).reshape(-1).astype(jnp.int32)
    sources = jnp.repeat(mid, TOP, axis=0)
    buffer = jnp.zeros((EXPERTS * N_EP * CAP, D), jnp.bfloat16).at[slot].set(sources)
    buffer = buffer.reshape(EXPERTS, N_EP * CAP, D)
    half_units = FE // N_TP

    def run_expert(items):
        rows_in, gate_w, up_w, down_w = items
        hidden = (jax.nn.silu(jnp.dot(rows_in, gate_w, preferred_element_type=jnp.float32)) * jnp.dot(rows_in, up_w, preferred_element_type=jnp.float32)).astype(jnp.bfloat16)
        total = jnp.zeros((rows_in.shape[0], D), jnp.float32)
        for part_idx in range(N_TP):
            lower = part_idx * half_units
            total = total + rounded(jnp.dot(hidden[:, lower:lower + half_units], down_w[lower:lower + half_units], preferred_element_type=jnp.float32))
        return total.astype(jnp.bfloat16)
    outputs = lax.map(run_expert, (buffer, expert_gate, expert_up, expert_down)).reshape(-1, D)
    picked = outputs[slot].astype(jnp.float32).reshape(BATCH, TOP, D)
    share = route_weights / lax.optimization_barrier(jnp.sum(route_weights, axis=1, keepdims=True)) * 2.5
    routed = lax.optimization_barrier(jnp.sum(share[..., None] * picked, axis=1))
    dense_hidden = (jax.nn.silu(jnp.dot(mid, dense_gate, preferred_element_type=jnp.float32)) * jnp.dot(mid, dense_up, preferred_element_type=jnp.float32)).astype(jnp.bfloat16)
    dense_out = jnp.dot(dense_hidden, dense_down, preferred_element_type=jnp.float32)
    mixed = (resid + routed + blend[:, None] * dense_out).astype(jnp.bfloat16)
    return (mixed, new_state)
```

```python
import functools

import jax
import jax.numpy as jnp
from jax import lax
from jax.experimental import pallas as pl
from jax.experimental.pallas import tpu as pltpu
from jax.sharding import Mesh
from jax.sharding import PartitionSpec as P

EP = ("ep_0", "ep_1", "ep_2")
EP_TP = ("ep_0", "ep_1", "ep_2", "tp")
NZ, NY, NX = 8, 4, 4
F32 = jnp.float32
BF16 = jnp.bfloat16
MESH_ID = pl.DeviceIdType.MESH
VMEM = pltpu.VMEM

D = 1536
ROWS = 8
WIDE = D + 128
AGA = slice(0, 512)
AGB = slice(512, 1024)
AGAB = slice(0, 1024)
AGC = slice(1024, WIDE)
CA = slice(0, 512)
CB = slice(512, 1024)
CC = slice(1024, 1536)
W = 512
N_COPIES = 192


def dot(a, b):
    return jnp.dot(a, b, preferred_element_type=F32)


def mixer_kernel(
    tok, gain, wq_h, wk_h, wv_h, dd, du, db, rd, ru, rb, hg, wo_h, st_h,
    part, st_out,
    wq, wk, wv, wo, st, dec_s, unit_s, ul_s, key_s, rec_s, val_s, mix_s, wsem, isem, osem,
):
    heads = st_h.shape[1]
    rows = tok.shape[0]
    loads = [
        pltpu.make_async_copy(src, dst, wsem.at[i])
        for i, (src, dst) in enumerate(((wk_h, wk), (wv_h, wv), (wq_h, wq), (wo_h, wo)))
    ]
    for load in loads[:3]:
        load.start()
    states = [pltpu.make_async_copy(st_h.at[:, h], st.at[h], isem.at[h]) for h in range(heads)]
    for copy in states:
        copy.start()
    loads[3].start()
    token_f = tok[...].astype(F32)
    scale = lax.rsqrt(jnp.mean(token_f * token_f, axis=-1, keepdims=True) + 1e-06)
    normed = (token_f * scale * gain[...]).astype(BF16)
    decay_low = jnp.tanh(dot(normed, dd[...])).astype(BF16)
    decay_in = db[...] + dot(decay_low, du[...])
    decay = jnp.exp(-0.6065306597126334 * jax.nn.sigmoid(decay_in))
    rate_low = dot(normed, rd[...]).astype(BF16)
    learn = jax.nn.sigmoid(rb[...] + dot(rate_low, ru[...]))
    loads[0].wait()
    key = dot(normed, wk[...]).astype(BF16).astype(F32)
    loads[1].wait()
    value = dot(normed, wv[...]).astype(BF16).astype(F32)
    loads[2].wait()
    rec = dot(normed, wq[...]).astype(BF16).astype(F32)
    value_t = jnp.transpose(value)
    for h in range(heads):
        lanes = slice(64 * h, 64 * h + 64)
        k = key[:, lanes]
        unit = k * lax.rsqrt(jnp.sum(k * k, axis=-1, keepdims=True) + 1e-06)
        key_s[h] = k
        unit_s[h] = unit
        ul_s[h] = unit * learn[:, lanes]
        dec_s[h] = decay[:, lanes]
        rec_s[h] = rec[:, lanes]
        val_s[h] = value_t[64 * h : 64 * h + 64, :]

    lane = lax.broadcasted_iota(jnp.int32, (64, 128), 1)

    def head(h, carry):
        pltpu.make_async_copy(st_h.at[:, h], st.at[h], isem.at[h]).wait()
        reads = jnp.zeros((64, 128), F32)
        for b in range(rows):
            prior = st[h, b]
            removed = jnp.sum(prior * unit_s[h, b : b + 1, :], axis=1, keepdims=True)
            new = (
                prior * dec_s[h, b : b + 1, :]
                - removed * ul_s[h, b : b + 1, :]
                + val_s[h, :, b : b + 1] * key_s[h, b : b + 1, :]
            )
            st[h, b] = new
            read = jnp.sum(new * rec_s[h, b : b + 1, :], axis=1, keepdims=True)
            reads = jnp.where(lane == b, read, reads)
        pltpu.make_async_copy(st.at[h], st_out.at[:, h], osem.at[h]).start()
        center = jnp.mean(reads, axis=0, keepdims=True)
        diff = reads - center
        spread = jnp.mean(diff * diff, axis=0, keepdims=True)
        mix_s[pl.ds(pl.multiple_of(h * 64, 64), 64), :] = diff * lax.rsqrt(spread + 0.00064) * hg[h]
        return carry

    lax.fori_loop(0, heads, head, 0)
    mixed = jnp.transpose(mix_s[...])[0:rows, :].astype(BF16)
    loads[3].wait()
    partial = dot(mixed, wo[...])
    part[0] = partial[0:8].astype(BF16)
    part[1] = partial[8:16].astype(BF16)

    def drain(h, carry):
        pltpu.make_async_copy(st.at[h], st_out.at[:, h], osem.at[h]).wait()
        return carry

    lax.fori_loop(0, heads, drain, 0)


def mixer(tokens, prior_state, first_gain, wq, wk, wv, dd, du, db, rd, ru, rb, hg, wo):
    rows, heads = prior_state.shape[:2]
    vm = pl.BlockSpec(memory_space=VMEM)
    hbm = pl.BlockSpec(memory_space=pl.ANY)
    inner = heads * 64
    small = VMEM((heads, rows, 64), F32)
    return pl.pallas_call(
        mixer_kernel,
        name="mixer",
        out_shape=(
            jax.ShapeDtypeStruct((2, rows // 2, D), BF16),
            jax.ShapeDtypeStruct(prior_state.shape, F32),
        ),
        in_specs=[vm, vm, hbm, hbm, hbm, vm, vm, vm, vm, vm, vm, vm, hbm, hbm],
        out_specs=(vm, hbm),
        scratch_shapes=[
            VMEM((D, inner), BF16), VMEM((D, inner), BF16), VMEM((D, inner), BF16),
            VMEM((inner, D), BF16), VMEM((heads, rows, 64, 64), F32),
            small, small, small, small, small,
            VMEM((heads, 64, rows), F32), VMEM((inner, 128), F32),
            pltpu.SemaphoreType.DMA((4,)),
            pltpu.SemaphoreType.DMA((heads,)),
            pltpu.SemaphoreType.DMA((heads,)),
        ],
    )(
        tokens, first_gain.reshape(1, D), wq, wk, wv, dd, du, db.reshape(1, inner), rd, ru,
        rb.reshape(1, inner), hg.reshape(heads, 64, 1), wo, prior_state,
    )


def exchange_kernel(
    part, tok, gain, ids, weights, blend, eg_h, eu_h, ed_h, dg_h, du_h, dd_h,
    out,
    full, made, w1, w2, eg, eu, dg, du, peer_part, fin, fin_in,
    ax1, axf, ay1, ayf, bx1, bxf, by1, byf, a2, b2, z3, r3, cz, c2, ry, c3, rx,
    send_sem, recv_sem, load_sem,
):
    z, y, x = (lax.axis_index(a) for a in EP)
    c = lax.axis_index("tp")
    expert = (z * NY + y) * NX + x
    count = [0]
    started = []

    def xa(d):
        return lax.rem(x + d + NX, NX)

    def ya(d):
        return lax.rem(y + d + NY, NY)

    def za(d):
        return lax.rem(z + d + NZ, NZ)

    def dev(dx=0, dy=0, dz=0, dc=0):
        return {
            "ep_0": za(dz) if dz else z,
            "ep_1": ya(dy) if dy else y,
            "ep_2": xa(dx) if dx else x,
            "tp": 1 - c if dc else c,
        }

    def send(src, dst, to):
        i = count[0]
        count[0] += 1
        copy = pltpu.make_async_remote_copy(
            src_ref=src, dst_ref=dst, send_sem=send_sem.at[i], recv_sem=recv_sem.at[i],
            device_id=to, device_id_type=MESH_ID,
        )
        copy.start()
        started.append(copy)
        return copy

    def rec(copies):
        for copy in copies:
            copy.wait_recv()

    loads = [
        pltpu.make_async_copy(src, dst, load_sem.at[i])
        for i, (src, dst) in enumerate(
            (
                (eg_h.at[0], eg), (eu_h.at[0], eu), (dg_h, dg), (du_h, du),
                (ed_h.at[0], w2.at[0, pl.ds(0, 192), :]),
                (dd_h, w2.at[0, pl.ds(192, 24), :]),
            )
        )
    ]
    for load in loads:
        load.start()

    peers = (
        [dev(dx=d) for d in range(1, NX)]
        + [dev(dy=d) for d in range(1, NY)]
        + [dev(dz=d) for d in range(1, NZ)]
        + [dev(dc=1)]
    )
    barrier = pltpu.get_barrier_semaphore()
    for peer in peers:
        pl.semaphore_signal(barrier, inc=1, device_id=peer, device_id_type=MESH_ID)
    pl.semaphore_wait(barrier, len(peers))

    swap = send(part.at[1 - c], peer_part, dev(dc=1))

    lane = lax.broadcasted_iota(jnp.int32, (ROWS, 128), 1)
    own_w = weights[c]
    own_ids = ids[c]
    share = own_w / jnp.sum(own_w, axis=1, keepdims=True) * 2.5
    shares = jnp.zeros((ROWS, 128), F32)
    for k in range(own_w.shape[1]):
        shares = shares + jnp.where(own_ids[:, k : k + 1] == lane, share[:, k : k + 1], 0.0)
    full[x, y, z, :, D:WIDE] = shares.astype(BF16)

    swap.wait_recv()
    attn = part[c].astype(F32) + peer_part[...].astype(F32)
    resid = (tok[c].astype(F32) + attn).astype(BF16).astype(F32)
    scale = lax.rsqrt(jnp.mean(resid * resid, axis=-1, keepdims=True) + 1e-06)
    full[x, y, z, :, 0:D] = (resid * scale * gain[...]).astype(BF16)

    def same(ref):
        return ref, ref

    zab = [send(*same(full.at[x, y, z, :, AGAB]), dev(dz=d)) for d in (1, 7, 2, 6, 3, 5, 4)]
    cx = [send(*same(full.at[x, y, z, :, AGC]), dev(dx=d)) for d in (1, 3, 2)]

    lo, hi = pl.ds(0, 256), pl.ds(256, 256)
    col = lax.broadcasted_iota(jnp.int32, (192, 256), 1)
    row = lax.broadcasted_iota(jnp.int32, (192, 256), 0)
    place_e = jnp.where(col == row, 1.0, 0.0).astype(BF16)
    col = lax.broadcasted_iota(jnp.int32, (24, 256), 1)
    row = lax.broadcasted_iota(jnp.int32, (24, 256), 0)
    place_d = jnp.where(col == row + 192, 1.0, 0.0).astype(BF16)
    for load in loads:
        load.wait()
    w2[0, 216:256, :] = jnp.zeros((40, D), BF16)
    w1[0, :, 0:256] = (dot(eg[...], place_e) + dot(dg[...], place_d)).astype(BF16)
    w1[0, :, 256:512] = (dot(eu[...], place_e) + dot(du[...], place_d)).astype(BF16)
    w_in = [send(w1.at[0], w1.at[1], dev(dc=1)), send(w2.at[0], w2.at[1], dev(dc=1))]

    rec(cx)
    cy = [send(*same(full.at[:, y, z, :, AGC]), dev(dy=d)) for d in (1, 3, 2)]
    rec(zab)

    def halves_out(ref_of, plus, minus):
        first = [send(*same(ref_of(0, 0)), plus), send(*same(ref_of(0, 1)), minus)]
        second = [send(*same(ref_of(0, 1)), plus), send(*same(ref_of(0, 0)), minus)]
        return first, second

    def halves_on(ref_of, first, plus, minus):
        first[0].wait_recv()
        a = send(*same(ref_of(-1, 0)), plus)
        first[1].wait_recv()
        b = send(*same(ref_of(1, 1)), minus)
        return [a, b]

    def a_y(d, half):
        return full.at[x, ya(d), pl.ds(4 * half, 4), :, AGA]

    def b_x(d, half):
        return full.at[xa(d), y, pl.ds(4 * half, 4), :, AGB]

    def a_x(d, half):
        return full.at[xa(d), pl.ds(2 * half, 2), :, :, AGA]

    def b_y(d, half):
        return full.at[pl.ds(2 * half, 2), ya(d), :, :, AGB]

    yp, ym, xp, xm = dev(dy=1), dev(dy=-1), dev(dx=1), dev(dx=-1)
    ay_1, ay_2 = halves_out(a_y, yp, ym)
    bx_1, bx_2 = halves_out(b_x, xp, xm)
    rec(cy)

    def c_z(d, q):
        return full.at[q, :, za(d), :, AGC]

    def ring_step(s):
        ups = range(4) if s < 4 else (0, 1)
        downs = range(4) if s < 4 else (2, 3)
        return ups, downs

    zp, zm = dev(dz=1), dev(dz=-1)
    ups = {q: send(*same(c_z(0, q)), zp) for q in range(4)}
    downs = {q: send(*same(c_z(0, q)), zm) for q in (2, 3, 0, 1)}

    def c_on(s, ups, downs):
        new_up, new_down = {}, {}
        for q, r in zip((0, 1, 2, 3), (2, 3, 0, 1)):
            ups[q].wait_recv()
            if s < 4 or q in (0, 1):
                new_up[q] = send(*same(c_z(-(s - 1), q)), zp)
            downs[r].wait_recv()
            if s < 4 or r in (2, 3):
                new_down[r] = send(*same(c_z(s - 1, r)), zm)
        return new_up, new_down

    ay_3 = halves_on(a_y, ay_1, yp, ym)
    bx_3 = halves_on(b_x, bx_1, xp, xm)
    ups, downs = c_on(2, ups, downs)
    rec(ay_2 + ay_3)
    ax_1, ax_2 = halves_out(a_x, xp, xm)
    rec(bx_2 + bx_3)
    by_1, by_2 = halves_out(b_y, yp, ym)
    ups, downs = c_on(3, ups, downs)
    ax_3 = halves_on(a_x, ax_1, xp, xm)
    by_3 = halves_on(b_y, by_1, yp, ym)
    ups, downs = c_on(4, ups, downs)
    rec(ax_2 + by_2 + ax_3 + by_3)
    rec(list(ups.values()) + list(downs.values()))
    rec(w_in)

    lane128 = lax.broadcasted_iota(jnp.int32, (256, 128), 1)
    lane256 = lax.broadcasted_iota(jnp.int32, (256, 256), 1)
    bvec = blend[...]

    def layers(xi):
        rows_in = full[xi].reshape(256, WIDE)
        mid = rows_in[:, 0:D]
        chosen = jnp.sum(
            jnp.where(lane128 == expert, rows_in[:, D:WIDE].astype(F32), 0.0), axis=1, keepdims=True
        )
        gate = lax.dot_general(mid, bvec, (((1,), (1,)), ((), ())), preferred_element_type=F32)
        level = jnp.where(lane256 < 192, chosen, jax.nn.sigmoid(gate[:, 0:1]))
        total = None
        for half in range(2):
            both = dot(mid, w1[half])
            g, u = both[:, 0:256], both[:, 256:512]
            hidden = (g * jax.nn.sigmoid(g) * u * level).astype(BF16)
            term = dot(hidden, w2[half])
            total = term if total is None else total + term
        made[xi] = total.astype(BF16).reshape(NY, NZ, ROWS, D)

    layers(xa(2))
    lower, upper = pl.ds(0, 4), pl.ds(4, 4)
    sx = [
        send(made.at[xa(2), :, lower, :, CA], ax1.at[0], xp),
        send(made.at[xa(2), :, upper, :, CA], ax1.at[1], xm),
    ]
    layers(xa(1))
    sx_free = [send(made.at[xa(1), :, upper, :, CA], axf.at[0, :, upper], xp)]
    layers(xa(-1))
    sx_free += [send(made.at[xa(-1), :, lower, :, CA], axf.at[1, :, lower], xm)]
    layers(x)

    def plus(a, b):
        return (a.astype(F32) + b.astype(F32)).astype(BF16)

    c_up, c_down = {}, {}
    c_up[1] = {q: send(made.at[q, :, za(4), :, CC], cz.at[0, 0, q], zp) for q in (0, 1)}
    c_down[1] = {q: send(made.at[q, :, za(4), :, CC], cz.at[1, 0, q], zm) for q in (2, 3)}
    c_up[2] = {q: send(made.at[q, :, za(3), :, CC], cz.at[0, 1, q], zp) for q in (2, 3)}
    c_down[2] = {q: send(made.at[q, :, za(-3), :, CC], cz.at[1, 1, q], zm) for q in (0, 1)}
    sy = [
        send(made.at[:, ya(2), lower, :, CB], by1.at[0], yp),
        send(made.at[:, ya(2), upper, :, CB], by1.at[1], ym),
    ]
    sy_free = [
        send(made.at[:, ya(1), upper, :, CB], byf.at[0, :, upper], yp),
        send(made.at[:, ya(-1), lower, :, CB], byf.at[1, :, lower], ym),
    ]
    sx[0].wait_recv()
    made[xa(1), :, 0:4, :, CA] = plus(made[xa(1), :, 0:4, :, CA], ax1[0])
    sx_free.append(send(made.at[xa(1), :, lower, :, CA], axf.at[0, :, lower], xp))
    sx[1].wait_recv()
    made[xa(-1), :, 4:8, :, CA] = plus(made[xa(-1), :, 4:8, :, CA], ax1[1])
    sx_free.append(send(made.at[xa(-1), :, upper, :, CA], axf.at[1, :, upper], xm))

    def c_back(s):
        for q, r in zip((0, 1, 2, 3), (2, 3, 0, 1)):
            if s > 2 or q in (0, 1):
                c_up[s - 1][q].wait_recv()
                made[q, :, za(5 - s), :, CC] = plus(made[q, :, za(5 - s), :, CC], cz[0, s - 2, q])
                c_up.setdefault(s, {})[q] = send(
                    made.at[q, :, za(5 - s), :, CC], cz.at[0, s - 1, q], zp
                )
            if s > 2 or r in (2, 3):
                c_down[s - 1][r].wait_recv()
                made[r, :, za(s - 5), :, CC] = plus(made[r, :, za(s - 5), :, CC], cz[1, s - 2, r])
                c_down.setdefault(s, {})[r] = send(
                    made.at[r, :, za(s - 5), :, CC], cz.at[1, s - 1, r], zm
                )

    c_back(2)
    sy[0].wait_recv()
    made[:, ya(1), 0:4, :, CB] = plus(made[:, ya(1), 0:4, :, CB], by1[0])
    sy_free.append(send(made.at[:, ya(1), lower, :, CB], byf.at[0, :, lower], yp))
    sy[1].wait_recv()
    made[:, ya(-1), 4:8, :, CB] = plus(made[:, ya(-1), 4:8, :, CB], by1[1])
    sy_free.append(send(made.at[:, ya(-1), upper, :, CB], byf.at[1, :, upper], ym))
    c_back(3)

    def three(a, b, d):
        return (a.astype(F32) + b.astype(F32) + d.astype(F32)).astype(BF16)

    def small_rs(buf, first, final, at, plus_to, minus_to):
        s = [
            send(buf.at[at(2), lower], first.at[0], plus_to),
            send(buf.at[at(2), upper], first.at[1], minus_to),
        ]
        f = [
            send(buf.at[at(1), upper], final.at[0, upper], plus_to),
            send(buf.at[at(-1), lower], final.at[1, lower], minus_to),
        ]
        return s, f

    def small_on(buf, first, final, at, plus_to, minus_to, s):
        s[0].wait_recv()
        buf[at(1), 0:4] = plus(buf[at(1), 0:4], first[0])
        f = [send(buf.at[at(1), lower], final.at[0, lower], plus_to)]
        s[1].wait_recv()
        buf[at(-1), 4:8] = plus(buf[at(-1), 4:8], first[1])
        f.append(send(buf.at[at(-1), upper], final.at[1, upper], minus_to))
        return f

    rec(sx_free)
    a2[...] = three(made[x, :, :, :, CA], axf[0], axf[1])
    a_s, a_f = small_rs(a2, ay1, ayf, ya, yp, ym)
    c_back(4)
    rec(sy_free)
    b2[...] = three(made[:, y, :, :, CB], byf[0], byf[1])
    b_s, b_f = small_rs(b2, bx1, bxf, xa, xp, xm)
    a_f += small_on(a2, ay1, ayf, ya, yp, ym, a_s)
    b_f += small_on(b2, bx1, bxf, xa, xp, xm, b_s)
    rec(list(c_up[4].values()) + list(c_down[4].values()))
    c2[...] = three(made[:, :, z, :, CC], cz[0, 3], cz[1, 3])
    sc = [send(c2.at[:, ya(d)], ry.at[d - 1], dev(dy=d)) for d in (1, 3, 2)]
    rec(a_f)
    z3[:, :, CA] = three(a2[y], ayf[0], ayf[1])
    rec(b_f)
    z3[:, :, CB] = three(b2[x], bxf[0], bxf[1])
    sz = [send(z3.at[za(d)], r3.at[d - 1], dev(dz=d)) for d in (4, 3, 5, 2, 6, 1, 7)]
    rec(sc)
    c3[...] = (
        c2[:, y].astype(F32) + ry[0].astype(F32) + ry[1].astype(F32) + ry[2].astype(F32)
    ).astype(BF16)
    sc = [send(c3.at[xa(d)], rx.at[d - 1], dev(dx=d)) for d in (1, 3, 2)]
    rec(sc)
    last = c3[x].astype(F32) + rx[0].astype(F32) + rx[1].astype(F32) + rx[2].astype(F32)
    fin[:, CC] = (resid[:, CC] + last).astype(BF16)
    rec(sz)
    early = z3[z].astype(F32)
    for d in range(NZ - 1):
        early = early + r3[d].astype(F32)
    fin[:, 0:1024] = (resid[:, 0:1024] + early).astype(BF16)

    half = D // 2
    other = pl.ds(pl.multiple_of((1 - c) * half, 128), half)
    mine = pl.ds(pl.multiple_of(c * half, 128), half)
    swap = send(fin.at[:, other], fin_in, dev(dc=1))
    out[c] = fin[:, mine]
    swap.wait_recv()
    out[1 - c] = fin_in[...]
    for copy in started:
        copy.wait_send()


def exchange(part, tokens, mid_gain, ids, weights, blend, eg, eu, ed, dg, du, dd):
    vm = pl.BlockSpec(memory_space=VMEM)
    hbm = pl.BlockSpec(memory_space=pl.ANY)
    return pl.pallas_call(
        exchange_kernel,
        name="exchange",
        out_shape=jax.ShapeDtypeStruct((2, ROWS, D // 2), BF16),
        in_specs=[vm] * 6 + [hbm] * 6,
        out_specs=vm,
        scratch_shapes=[
            VMEM((NX, NY, NZ, ROWS, WIDE), BF16),
            VMEM((NX, NY, NZ, ROWS, D), BF16),
            VMEM((2, D, 512), BF16),
            VMEM((2, 256, D), BF16),
            VMEM((D, 192), BF16), VMEM((D, 192), BF16),
            VMEM((D, 24), BF16), VMEM((D, 24), BF16),
            VMEM((ROWS, D), BF16), VMEM((ROWS, D), BF16), VMEM((ROWS, D // 2), BF16),
            VMEM((2, NY, 4, ROWS, W), BF16), VMEM((2, NY, NZ, ROWS, W), BF16),
            VMEM((2, 4, ROWS, W), BF16), VMEM((2, NZ, ROWS, W), BF16),
            VMEM((2, 4, ROWS, W), BF16), VMEM((2, NZ, ROWS, W), BF16),
            VMEM((2, NX, 4, ROWS, W), BF16), VMEM((2, NX, NZ, ROWS, W), BF16),
            VMEM((NY, NZ, ROWS, W), BF16), VMEM((NX, NZ, ROWS, W), BF16),
            VMEM((NZ, ROWS, 2 * W), BF16), VMEM((NZ - 1, ROWS, 2 * W), BF16),
            VMEM((2, 4, NX, NY, ROWS, W), BF16), VMEM((NX, NY, ROWS, W), BF16),
            VMEM((NY - 1, NX, ROWS, W), BF16), VMEM((NX, ROWS, W), BF16),
            VMEM((NX - 1, ROWS, W), BF16),
            pltpu.SemaphoreType.DMA((N_COPIES,)),
            pltpu.SemaphoreType.DMA((N_COPIES,)),
            pltpu.SemaphoreType.DMA((6,)),
        ],
        compiler_params=pltpu.CompilerParams(collective_id=0, has_side_effects=True),
    )(part, tokens, mid_gain, ids, weights, blend, eg, eu, ed, dg, du, dd)


def shards(
    tokens, prior_state, first_gain, query_weight, key_weight, value_weight, decay_down, decay_up,
    decay_base, rate_down, rate_up, rate_base, head_gain, out_weight, mid_gain, route_ids,
    route_weights, expert_gate, expert_up, expert_down, dense_gate, dense_up, dense_down,
    blend_vector,
):
    part, new_state = mixer(
        tokens, prior_state, first_gain, query_weight, key_weight, value_weight, decay_down,
        decay_up, decay_base, rate_down, rate_up, rate_base, head_gain, out_weight,
    )
    top = route_ids.shape[1]
    mixed = exchange(
        part, tokens.reshape(2, ROWS, D), mid_gain.reshape(1, D), route_ids.reshape(2, ROWS, top),
        route_weights.reshape(2, ROWS, top), jnp.broadcast_to(blend_vector[None, :], (8, D)),
        expert_gate, expert_up, expert_down, dense_gate, dense_up, dense_down,
    )
    return (mixed.reshape(2 * ROWS, D // 2), new_state)


def solution(mesh):
    split = Mesh(mesh.devices.reshape(NZ, NY, NX, mesh.shape["tp"]), EP_TP)
    in_specs = (
        P(EP, None),
        P(EP, "tp", None, None),
        P(),
        P(None, "tp"),
        P(None, "tp"),
        P(None, "tp"),
        P(),
        P(None, "tp"),
        P("tp"),
        P(),
        P(None, "tp"),
        P("tp"),
        P("tp"),
        P("tp", None),
        P(),
        P(EP, None),
        P(EP, None),
        P(EP, None, "tp"),
        P(EP, None, "tp"),
        P(EP, "tp", None),
        P(None, EP_TP),
        P(None, EP_TP),
        P(EP_TP, None),
        P(),
    )
    out_specs = (P(EP, "tp"), P(EP, "tp", None, None))
    return jax.shard_map(
        shards, mesh=split, in_specs=in_specs, out_specs=out_specs, check_vma=False
    )
```

```python
import math

import jax
import jax.numpy as jnp
from jax import lax
from jax.experimental import pallas as pl
from jax.experimental.pallas import tpu as pltpu
from jax.sharding import Mesh
from jax.sharding import PartitionSpec as P

EP = ("ep_0", "ep_1", "ep_2")
EP_TP = ("ep_0", "ep_1", "ep_2", "tp")
NZ, NY, NX = 8, 4, 4
F32 = jnp.float32
BF16 = jnp.bfloat16
MESH_ID = pl.DeviceIdType.MESH
VMEM = pltpu.VMEM

D = 1536
ROWS = 8
WIDE = D + 128
AGA = slice(0, 512)
AGB = slice(512, 1024)
AGAB = slice(0, 1024)
AGC = slice(1024, WIDE)
CA = slice(0, 512)
CB = slice(512, 1024)
CC = slice(1024, 1536)
W = 512
N_SEND, N_RECV, N_TILES = 10, 117, 1152


def dot(a, b):
    return jnp.dot(a, b, preferred_element_type=F32)


def dot_t(a, b):
    return lax.dot_general(a, b, (((1,), (1,)), ((), ())), preferred_element_type=F32)


def flat(ref):
    return jnp.concatenate([ref[j : j + 1, :] for j in range(ref.shape[0])], axis=1)


scope = jax.named_scope


def mixer_kernel(
    tok, gain, wq_h, wk_h, wv_h, dd, du, db, rd, ru, rb, hg, wo_h, st_h,
    part, st_out,
    wq, wk, wv, wo, st, dec_s, left_s, right_s, val_s, both_s, wsem, isem, osem,
):
    heads = st_h.shape[1]
    rows = tok.shape[0]
    loads = [
        pltpu.make_async_copy(src, dst, wsem.at[i])
        for i, (src, dst) in enumerate(((wk_h, wk), (wv_h, wv), (wq_h, wq), (wo_h, wo)))
    ]
    for load in loads[:3]:
        load.start()
    states = [pltpu.make_async_copy(st_h.at[:, h], st.at[h], isem.at[h]) for h in range(heads)]
    for copy in states:
        copy.start()
    loads[3].start()
    with scope("m_norm"):
        token_f = tok[...].astype(F32)
        scale = lax.rsqrt(jnp.mean(token_f * token_f, axis=-1, keepdims=True) + 1e-06)
        normed = (token_f * scale * flat(gain)).astype(BF16)
        decay_low = jnp.tanh(dot_t(normed, dd[...])).astype(BF16)
        decay_in = flat(db) + dot(decay_low, du[...])
        decay = jnp.exp(-0.6065306597126334 * jax.nn.sigmoid(decay_in))
        rate_low = dot_t(normed, rd[...]).astype(BF16)
        learn = jax.nn.sigmoid(flat(rb) + dot(rate_low, ru[...]))
    with scope("m_qkv"):
        loads[0].wait()
        key = dot(normed, wk[...]).astype(BF16).astype(F32)
        loads[1].wait()
        value = dot(normed, wv[...]).astype(BF16).astype(F32)
        loads[2].wait()
        rec = dot(normed, wq[...]).astype(BF16).astype(F32)
    with scope("m_prep"):
        val_s[...] = jnp.transpose(jnp.concatenate([jnp.zeros_like(value), value], axis=0)).reshape(
            heads, 64, 2 * rows
        )
        taken, given = [], []
        for h in range(heads):
            lanes = slice(64 * h, 64 * h + 64)
            k, r, d = key[:, lanes], rec[:, lanes], decay[:, lanes]
            unit = k * lax.rsqrt(jnp.sum(k * k, axis=-1, keepdims=True) + 1e-06)
            rate = unit * learn[:, lanes]
            dec_s[h] = d
            left_s[h, 0:rows] = unit.astype(BF16)
            left_s[h, rows : 2 * rows] = (d * r).astype(BF16)
            right_s[h, 0:rows] = rate.astype(BF16)
            right_s[h, rows : 2 * rows] = k.astype(BF16)
            taken.append(jnp.sum(rate * r, axis=-1, keepdims=True))
            given.append(jnp.sum(k * r, axis=-1, keepdims=True))

    lane = lax.broadcasted_iota(jnp.int32, (64, 2 * rows), 1)

    def head(h, carry):
        pltpu.make_async_copy(st_h.at[:, h], st.at[h], isem.at[h]).wait()
        prior = st[h].reshape(rows * 64, 64)
        products = dot_t(prior.astype(BF16), left_s[h])
        own = jnp.zeros((64, 2 * rows), F32)
        values = val_s[h]
        outer = []
        for b in range(rows):
            here = products[64 * b : 64 * b + 64]
            first, second = lane == b, lane == rows + b
            own = jnp.where(first | second, here, own)
            outer.append(
                jnp.where(first, -here, jnp.where(second, values, 0.0)).astype(BF16)
            )
        change = dot(jnp.concatenate(outer, axis=0), right_s[h])
        for b in range(rows):
            part_b = slice(64 * b, 64 * b + 64)
            st[h, b] = prior[part_b] * dec_s[h, b : b + 1, :] + change[part_b]
        both_s[pl.ds(pl.multiple_of(h * 64, 64), 64), :] = own
        pltpu.make_async_copy(st.at[h], st_out.at[:, h], osem.at[h]).start()
        return carry

    with scope("m_state"):
        lax.fori_loop(0, heads, head, 0)
    with scope("m_out"):
        both = jnp.transpose(both_s[...])
        mixed = []
        for h in range(heads):
            lanes = slice(64 * h, 64 * h + 64)
            read = (
                both[rows : 2 * rows, lanes]
                - both[0:rows, lanes] * taken[h]
                + value[:, lanes] * given[h]
            )
            diff = read - jnp.mean(read, axis=-1, keepdims=True)
            spread = jnp.mean(diff * diff, axis=-1, keepdims=True)
            mixed.append(diff * lax.rsqrt(spread + 0.00064))
        mixed = (jnp.concatenate(mixed, axis=1) * flat(hg)).astype(BF16)
        loads[3].wait()
        partial = dot(mixed, wo[...])
        part[0] = partial[0:8].astype(BF16)
        part[1] = partial[8:16].astype(BF16)

    def drain(h, carry):
        pltpu.make_async_copy(st.at[h], st_out.at[:, h], osem.at[h]).wait()
        return carry

    with scope("m_drain"):
        lax.fori_loop(0, heads, drain, 0)


def mixer(tokens, prior_state, first_gain, wq, wk, wv, dd, du, db, rd, ru, rb, hg, wo):
    rows, heads = prior_state.shape[:2]
    vm = pl.BlockSpec(memory_space=VMEM)
    hbm = pl.BlockSpec(memory_space=pl.ANY)
    inner = heads * 64
    return pl.pallas_call(
        mixer_kernel,
        name="mixer",
        out_shape=(
            jax.ShapeDtypeStruct((2, rows // 2, D), BF16),
            jax.ShapeDtypeStruct(prior_state.shape, F32),
        ),
        in_specs=[vm, vm, hbm, hbm, hbm, vm, vm, vm, vm, vm, vm, vm, hbm, hbm],
        out_specs=(vm, hbm),
        scratch_shapes=[
            VMEM((D, inner), BF16), VMEM((D, inner), BF16), VMEM((D, inner), BF16),
            VMEM((inner, D), BF16), VMEM((heads, rows, 64, 64), F32),
            VMEM((heads, rows, 64), F32),
            VMEM((heads, 2 * rows, 64), BF16), VMEM((heads, 2 * rows, 64), BF16),
            VMEM((heads, 64, 2 * rows), F32), VMEM((inner, 2 * rows), F32),
            pltpu.SemaphoreType.DMA((4,)),
            pltpu.SemaphoreType.DMA((heads,)),
            pltpu.SemaphoreType.DMA((heads,)),
        ],
    )(
        tokens, first_gain.reshape(-1, 128), wq, wk, wv, dd.T, du, db.reshape(-1, 128), rd.T, ru,
        rb.reshape(-1, 128), hg.reshape(-1, 128), wo, prior_state,
    )


class Group:
    def __init__(self, index):
        self.index, self.tiles = index, 0


AROUND = (2, 1, -1, 0)
UP4, DOWN4 = (2, 1), (-1, 0)


def exchange_kernel(
    part, tok, gain, ids, weights, blend, eg_h, eu_h, ed_h, dg_h, du_h, dd_h,
    out,
    full, made, w1, w2, shares_s, peer_part, res_s, res_in,
    ax1, axf, ay1, ayf, bx1, bxf, by1, byf, a2, b2, z3, r3, cz, c2, ry, c3, rx, tiles,
    send_sem, recv_sem, load_sem,
):
    z, y, x = (lax.axis_index(a) for a in EP)
    c = lax.axis_index("tp")
    expert = (z * NY + y) * NX + x
    families, groups = [], []

    def xa(d):
        return lax.rem(x + d + NX, NX)

    def ya(d):
        return lax.rem(y + d + NY, NY)

    def za(d):
        return lax.rem(z + d + NZ, NZ)

    def dev(dx=0, dy=0, dz=0, dc=0):
        return {
            "ep_0": za(dz) if dz else z,
            "ep_1": ya(dy) if dy else y,
            "ep_2": xa(dx) if dx else x,
            "tp": 1 - c if dc else c,
        }

    def family():
        families.append(Group(len(families)))
        return families[-1]

    def group():
        groups.append(Group(len(groups)))
        return groups[-1]

    def send(src, dst, to, sent, got):
        size = math.prod(src.shape) // (ROWS * 128)
        sent.tiles += size
        got.tiles += size
        pltpu.make_async_remote_copy(
            src_ref=src, dst_ref=dst, send_sem=send_sem.at[sent.index],
            recv_sem=recv_sem.at[got.index], device_id=to, device_id_type=MESH_ID,
        ).start()
        return got

    def all_of(g):
        view = tiles.at[pl.ds(0, g.tiles)]
        return pltpu.make_async_remote_copy(
            src_ref=view, dst_ref=view,
            send_sem=send_sem.at[g.index if g in families else 0],
            recv_sem=recv_sem.at[g.index if g in groups else 0],
            device_id=dev(dc=1), device_id_type=MESH_ID,
        )

    def arrive(*some):
        for g in some:
            all_of(g).wait_recv()

    pieces = [
        (eg_h.at[0], w1.at[0, pl.ds(0, 192), :]),
        (dg_h, w1.at[0, pl.ds(192, 24), :]),
        (eu_h.at[0], w1.at[0, pl.ds(256, 192), :]),
        (du_h, w1.at[0, pl.ds(448, 24), :]),
    ]
    for k, at in enumerate((0, 768, 256, 1024, 512, 1280)):
        here, there = pl.ds(256 * k, 256), pl.ds(at, 256)
        pieces.append((ed_h.at[0, :, there], w2.at[0, pl.ds(0, 192), here]))
        pieces.append((dd_h.at[:, there], w2.at[0, pl.ds(192, 24), here]))
    loads = [pltpu.make_async_copy(src, dst, load_sem.at[i]) for i, (src, dst) in enumerate(pieces)]
    for load in loads:
        load.start()

    with scope("barrier"):
        peers = (
            [dev(dx=d, dc=e) for d in range(1, NX) for e in (0, 1)]
            + [dev(dy=d) for d in range(1, NY)]
            + [dev(dz=d, dc=e) for d in range(1, NZ) for e in (0, 1)]
            + [dev(dc=1)]
        )
        barrier = pltpu.get_barrier_semaphore()
        for peer in peers:
            pl.semaphore_signal(barrier, inc=1, device_id=peer, device_id_type=MESH_ID)
        pl.semaphore_wait(barrier, len(peers))

    near = family()
    swap = send(part.at[1 - c], peer_part, dev(dc=1), near, group())

    with scope("shares"):
        own_w = weights[...]
        share = own_w / jnp.sum(own_w, axis=0, keepdims=True) * 2.5
        sub = lax.broadcasted_iota(jnp.int32, (128, 2 * ROWS), 0)
        shares = jnp.zeros((128, 2 * ROWS), F32)
        for k in range(own_w.shape[0]):
            shares = shares + jnp.where(ids[k : k + 1, :] == sub, share[k : k + 1, :], 0.0)
        shares_s[...] = jnp.transpose(shares).reshape(2, ROWS, 128)
        full[x, y, z, :, D:WIDE] = shares_s[c].astype(BF16)
        first_row = lax.broadcasted_iota(jnp.int32, (ROWS, D), 0) == 0
        w1[0, 216:224, :] = jnp.where(first_row, blend[...].astype(F32).reshape(1, D), 0.0).astype(BF16)
        w1[0, 224:256, :] = jnp.zeros((32, D), BF16)
        w1[0, 472:512, :] = jnp.zeros((40, D), BF16)
        w2[0, 216:256, :] = jnp.zeros((40, D), BF16)

    with scope("mid"):
        arrive(swap)
        attn = part[c].astype(F32) + peer_part[...].astype(F32)
        resid_bf = (tok[c].astype(F32) + attn).astype(BF16)
        resid = resid_bf.astype(F32)
        scale = lax.rsqrt(jnp.mean(resid * resid, axis=-1, keepdims=True) + 1e-06)
        full[x, y, z, :, 0:D] = (resid * scale * flat(gain)).astype(BF16)
        res_s[0] = resid_bf[:, 0:768]
        res_s[1] = resid_bf[:, 768:1536]

    yp, ym, xp, xm = dev(dy=1), dev(dy=-1), dev(dx=1), dev(dx=-1)
    zp, zm = dev(dz=1), dev(dz=-1)
    fam_z, fam_a, fam_b, fam_c = family(), family(), family(), family()

    zab = group()
    for d in (4, 3, 5, 2, 6, 1, 7):
        ref = full.at[x, y, z, :, AGAB]
        send(ref, ref, dev(dz=d), fam_z, zab)
    cx = group()
    for d in (2, 1, 3):
        ref = full.at[x, y, z, :, AGC]
        send(ref, ref, dev(dx=d), fam_z, cx)

    resid_in = send(res_s.at[1 - c], res_in, dev(dc=1), near, group())
    with scope("w_load"):
        for load in loads:
            load.wait()
    w_fam, w_in = family(), group()
    send(w1.at[0], w1.at[1], dev(dc=1), w_fam, w_in)
    send(w2.at[0], w2.at[1], dev(dc=1), w_fam, w_in)

    def halves_out(ref_of, up, down, fam, first, rest):
        for at, half, to in ((0, 0, up), (1, 1, down), (0, 1, up), (1, 0, down)):
            ref = ref_of(0, half)
            send(ref, ref, to, fam, first[at] if half == at else rest)

    def halves_on(ref_of, up, down, fam, first, last):
        for at, d, to in ((0, -1, up), (1, 1, down)):
            arrive(first[at])
            ref = ref_of(d, at)
            send(ref, ref, to, fam, last)

    def a_y(d, half):
        return full.at[x, ya(d), pl.ds(4 * half, 4), :, AGA]

    def b_x(d, half):
        return full.at[xa(d), y, pl.ds(4 * half, 4), :, AGB]

    def a_x(j):
        return lambda d, half: full.at[xa(d), ya(j), pl.ds(4 * half, 4), :, AGA]

    def b_y(i):
        return lambda d, half: full.at[xa(i), ya(d), pl.ds(4 * half, 4), :, AGB]

    ay_first, ay_rest, ay_last = (group(), group()), group(), group()
    bx_first, bx_rest, bx_last = (group(), group()), group(), group()
    ax_first = {j: (group(), group()) for j in AROUND}
    by_first = {i: (group(), group()) for i in AROUND}
    ax_rest, by_rest = group(), group()

    def ab_out(j):
        halves_out(a_x(j), xp, xm, fam_a, ax_first[j], ax_rest)
        halves_out(b_y(j), yp, ym, fam_b, by_first[j], by_rest)

    def ab_on(j):
        halves_on(a_x(j), xp, xm, fam_a, ax_first[j], ax_rest)
        halves_on(b_y(j), yp, ym, fam_b, by_first[j], by_rest)

    up_in = {(s, q): group() for s in (1, 2, 3) for q in AROUND}
    down_in = {(s, q): group() for s in (1, 2, 3) for q in AROUND}
    c_last = group()

    def c_z(s, q):
        if s > 1:
            arrive(up_in[s - 1, q])
        if s < 4 or q in UP4:
            ref = full.at[:, ya(q), za(1 - s), :, AGC]
            send(ref, ref, zp, fam_c, up_in[s, q] if s < 4 else c_last)
        if s > 1:
            arrive(down_in[s - 1, q])
        if s < 4 or q in DOWN4:
            ref = full.at[:, ya(q), za(s - 1), :, AGC]
            send(ref, ref, zm, fam_c, down_in[s, q] if s < 4 else c_last)

    with scope("ag_cx"):
        arrive(cx)
        cy = {d: group() for d in (1, 3, 2)}
        for d in (1, 3, 2):
            ref = full.at[:, y, z, :, AGC]
            send(ref, ref, dev(dy=d), fam_c, cy[d])
        c_z(1, 0)
    with scope("ag_zab"):
        arrive(zab)
        halves_out(a_y, yp, ym, fam_a, ay_first, ay_rest)
        halves_out(b_x, xp, xm, fam_b, bx_first, bx_rest)
        ab_out(0)
    with scope("ag_cy"):
        arrive(cy[1], cy[3])
        c_z(1, 1)
        c_z(1, -1)
        arrive(cy[2])
        c_z(1, 2)
        c_z(2, 0)
    with scope("ag_ab_half"):
        halves_on(a_y, yp, ym, fam_a, ay_first, ay_last)
        halves_on(b_x, xp, xm, fam_b, bx_first, bx_last)
    with scope("ag_ab_rest"):
        arrive(ay_rest, bx_rest)
        ab_out(1)
        ab_out(-1)
        ab_on(0)
    with scope("ag_c2"):
        c_z(2, 1)
        c_z(2, -1)
        c_z(3, 0)
        c_z(2, 2)
    with scope("ag_ab_last"):
        arrive(ay_last, bx_last)
        ab_out(2)
    with scope("ag_c3"):
        c_z(3, 1)
        c_z(3, -1)
        c_z(4, 0)
    with scope("ag_ab_1"):
        ab_on(1)
        ab_on(-1)
    with scope("ag_c4"):
        c_z(3, 2)
        c_z(4, 1)
        c_z(4, -1)
    with scope("ag_ab_2"):
        ab_on(2)
    with scope("ag_c4_2"):
        c_z(4, 2)
    with scope("ag_end_ab"):
        arrive(ax_rest, by_rest)
    with scope("ag_end_c"):
        arrive(c_last, w_in)

    lane128 = lax.broadcasted_iota(jnp.int32, (256, 128), 1)
    lane256 = lax.broadcasted_iota(jnp.int32, (256, 256), 1)

    def layers(yi):
        rows_in = full[:, yi].reshape(256, WIDE)
        mid = rows_in[:, 0:D]
        chosen = jnp.sum(
            jnp.where(lane128 == expert, rows_in[:, D:WIDE].astype(F32), 0.0), axis=1, keepdims=True
        )
        both = dot_t(mid, w1[0])
        level = jnp.where(lane256 < 192, chosen, jax.nn.sigmoid(both[:, 216:217]))
        total = None
        for half in range(2):
            if half:
                both = dot_t(mid, w1[1])
            g, u = both[:, 0:256], both[:, 256:512]
            hidden = (g * jax.nn.sigmoid(g) * u * level).astype(BF16)
            term = dot(hidden, w2[half])
            total = term if total is None else total + term
        made[:, yi] = total.astype(BF16).reshape(NX, NZ, ROWS, D)

    def plus(*terms):
        total = terms[0].astype(F32)
        for term in terms[1:]:
            total = total + term.astype(F32)
        return total.astype(BF16)

    lower, upper = pl.ds(0, 4), pl.ds(4, 4)
    rs_a, rs_b, rs_c, rs_z = family(), family(), family(), family()
    slot = {j: k for k, j in enumerate(AROUND)}
    ax_one = {j: (group(), group()) for j in AROUND}
    ax_fin = {j: group() for j in AROUND}
    by_one = {i: (group(), group()) for i in AROUND}
    by_fin = {i: group() for i in AROUND}

    def a_start(j):
        k, yj = slot[j], ya(j)
        send(made.at[xa(2), yj, lower, :, CA], ax1.at[k, 0], xp, rs_a, ax_one[j][0])
        send(made.at[xa(2), yj, upper, :, CA], ax1.at[k, 1], xm, rs_a, ax_one[j][1])
        send(made.at[xa(1), yj, upper, :, CA], axf.at[k, 0, upper], xp, rs_a, ax_fin[j])
        send(made.at[xa(-1), yj, lower, :, CA], axf.at[k, 1, lower], xm, rs_a, ax_fin[j])

    def a_on(j):
        k, yj = slot[j], ya(j)
        arrive(ax_one[j][0])
        made[xa(1), yj, 0:4, :, CA] = plus(made[xa(1), yj, 0:4, :, CA], ax1[k, 0])
        send(made.at[xa(1), yj, lower, :, CA], axf.at[k, 0, lower], xp, rs_a, ax_fin[j])
        arrive(ax_one[j][1])
        made[xa(-1), yj, 4:8, :, CA] = plus(made[xa(-1), yj, 4:8, :, CA], ax1[k, 1])
        send(made.at[xa(-1), yj, upper, :, CA], axf.at[k, 1, upper], xm, rs_a, ax_fin[j])

    def a_end(j):
        k = slot[j]
        arrive(ax_fin[j])
        return plus(made[x, ya(j), :, :, CA], axf[k, 0], axf[k, 1])

    def b_start(i):
        k, xi = slot[i], xa(i)
        send(made.at[xi, ya(2), lower, :, CB], by1.at[k, 0], yp, rs_b, by_one[i][0])
        send(made.at[xi, ya(2), upper, :, CB], by1.at[k, 1], ym, rs_b, by_one[i][1])

    def b_free(i, d):
        k, xi = slot[i], xa(i)
        if d > 0:
            send(made.at[xi, ya(1), upper, :, CB], byf.at[k, 0, upper], yp, rs_b, by_fin[i])
        else:
            send(made.at[xi, ya(-1), lower, :, CB], byf.at[k, 1, lower], ym, rs_b, by_fin[i])

    def b_on(i):
        k, xi = slot[i], xa(i)
        arrive(by_one[i][0])
        made[xi, ya(1), 0:4, :, CB] = plus(made[xi, ya(1), 0:4, :, CB], by1[k, 0])
        send(made.at[xi, ya(1), lower, :, CB], byf.at[k, 0, lower], yp, rs_b, by_fin[i])
        arrive(by_one[i][1])
        made[xi, ya(-1), 4:8, :, CB] = plus(made[xi, ya(-1), 4:8, :, CB], by1[k, 1])
        send(made.at[xi, ya(-1), upper, :, CB], byf.at[k, 1, upper], ym, rs_b, by_fin[i])

    def b_end(i):
        k = slot[i]
        arrive(by_fin[i])
        return plus(made[xa(i), y, :, :, CB], byf[k, 0], byf[k, 1])

    class Second:
        def __init__(self, buf, one, fin, up, down, fam):
            self.buf, self.one, self.fin, self.up, self.down, self.fam = buf, one, fin, up, down, fam
            self.got, self.end = (group(), group()), group()

        def put(self, j, block):
            buf, k = self.buf, slot[j]
            buf[k] = block
            if j == 2:
                send(buf.at[k, lower], self.one.at[0], self.up, self.fam, self.got[0])
                send(buf.at[k, upper], self.one.at[1], self.down, self.fam, self.got[1])
            elif j == 1:
                send(buf.at[k, upper], self.fin.at[0, upper], self.up, self.fam, self.end)
            elif j == -1:
                send(buf.at[k, lower], self.fin.at[1, lower], self.down, self.fam, self.end)

        def on(self, j):
            buf, k = self.buf, slot[j]
            if j == 1:
                arrive(self.got[0])
                buf[k, 0:4] = plus(buf[k, 0:4], self.one[0])
                send(buf.at[k, lower], self.fin.at[0, lower], self.up, self.fam, self.end)
            else:
                arrive(self.got[1])
                buf[k, 4:8] = plus(buf[k, 4:8], self.one[1])
                send(buf.at[k, upper], self.fin.at[1, upper], self.down, self.fam, self.end)

        def sums(self):
            arrive(self.end)
            return plus(self.buf[slot[0]], self.fin[0], self.fin[1])

    c_up = {(s, q): group() for s in (1, 2, 3) for q in AROUND if s > 1 or q in UP4}
    c_down = {(s, q): group() for s in (1, 2, 3) for q in AROUND if s > 1 or q in DOWN4}
    c_fin = {q: group() for q in AROUND}

    def c_send(s, q, up):
        way, to = (0, zp) if up else (1, zm)
        at = za(5 - s) if up else za(s - 5)
        got = c_fin[q] if s == 4 else (c_up if up else c_down)[s, q]
        send(made.at[:, ya(q), at, :, CC], cz.at[way, s - 1, slot[q]], to, rs_c, got)

    def c_start(q):
        c_send(1, q, q in UP4)
        c_send(2, q, q in DOWN4)

    def c_on(s, q):
        for up, got in ((True, c_up), (False, c_down)):
            if (s - 1, q) in got:
                at = za(5 - s) if up else za(s - 5)
                arrive(got[s - 1, q])
                made[:, ya(q), at, :, CC] = plus(
                    made[:, ya(q), at, :, CC], cz[0 if up else 1, s - 2, slot[q]]
                )
                c_send(s, q, up)

    cy_in = group()

    def c_end(q):
        k = slot[q]
        arrive(c_fin[q])
        c2[k] = plus(made[:, ya(q), z, :, CC], cz[0, 3, k], cz[1, 3, k])
        if q:
            send(c2.at[k], ry.at[k], dev(dy=q), rs_c, cy_in)

    a_next = Second(a2, ay1, ayf, yp, ym, rs_a)
    b_next = Second(b2, bx1, bxf, xp, xm, rs_b)

    with scope("rs_m2"):
        layers(ya(2))
        a_start(2)
        c_start(2)
        for i in AROUND:
            b_start(i)
    with scope("rs_m1"):
        layers(ya(1))
        a_start(1)
        c_start(1)
        for i in AROUND:
            b_free(i, 1)
    with scope("rs_m-1"):
        layers(ya(-1))
        a_start(-1)
        c_start(-1)
        for i in AROUND:
            b_free(i, -1)
    with scope("rs_on2"):
        c_on(2, 2)
        a_on(2)
    with scope("rs_m0"):
        layers(y)
        a_start(0)
        c_start(0)
    with scope("rs_b_on"):
        c_on(3, 2)
        b_on(2)
        c_on(2, 1)
        b_on(1)
    with scope("rs_a_on"):
        a_on(1)
        c_on(2, -1)
        a_on(-1)
        b_on(-1)
        b_on(0)
    with scope("rs_c_a"):
        c_on(4, 2)
        c_on(3, 1)
        c_on(2, 0)
        c_on(3, -1)
    with scope("rs_a_end2"):
        a_next.put(2, a_end(2))
        a_on(0)
        b_next.put(2, b_end(2))
    with scope("rs_a_end1"):
        a_next.put(1, a_end(1))
        c_on(4, 1)
        c_on(3, 0)
        c_on(4, -1)
        a_next.put(-1, a_end(-1))
    with scope("rs_b_end1"):
        b_next.put(1, b_end(1))
        c_end(2)
        a_next.on(1)
        b_next.put(-1, b_end(-1))
    with scope("rs_next"):
        a_next.on(-1)
        c_on(4, 0)
        b_next.on(1)
        b_next.on(-1)
    with scope("rs_c_end"):
        c_end(1)
        c_end(-1)
    with scope("rs_ab_0"):
        a_next.put(0, a_end(0))
        b_next.put(0, b_end(0))

    z_same, z_other, x_in = group(), group(), group()
    with scope("rs_z_out"):
        sums_a = a_next.sums()
        z3[0, :, :, 0:256] = sums_a[:, :, 0:256]
        z3[1, :, :, 0:256] = sums_a[:, :, 256:512]
        sums_b = b_next.sums()
        z3[0, :, :, 256:512] = sums_b[:, :, 0:256]
        z3[1, :, :, 256:512] = sums_b[:, :, 256:512]
        for d in (4, 3, 5, 2, 6, 1, 7, 0):
            send(z3.at[1 - c, za(d)], r3.at[1, d], dev(dz=d, dc=1), rs_z, z_other)
            if d:
                send(z3.at[c, za(d)], r3.at[0, d], dev(dz=d), rs_z, z_same)
    with scope("rs_c_x"):
        c_end(0)
        arrive(cy_in)
        sums_c = plus(*(ry[slot[q]] for q in (1, -1, 2)), c2[slot[0]])
        c3[0] = sums_c[:, :, 0:256]
        c3[1] = sums_c[:, :, 256:512]
        for d in (2, 1, 3, 0):
            send(c3.at[1 - c, xa(d)], rx.at[1, d], dev(dx=d, dc=1), rs_z, x_in)
            if d:
                send(c3.at[c, xa(d)], rx.at[0, d], dev(dx=d), rs_z, x_in)
    with scope("rs_fin"):
        arrive(resid_in, z_same)
        total = res_s[c, :, 0:512].astype(F32) + z3[c, z].astype(F32)
        for d in range(1, NZ):
            total = total + r3[0, d].astype(F32)
        out[c, :, 0:512] = total.astype(BF16)
        arrive(z_other)
        total = res_in[:, 0:512].astype(F32)
        for d in range(NZ):
            total = total + r3[1, d].astype(F32)
        out[1 - c, :, 0:512] = total.astype(BF16)
        arrive(x_in)
        out[c, :, 512:768] = plus(res_s[c, :, 512:768], c3[c, x], rx[0, 1], rx[0, 2], rx[0, 3])
        out[1 - c, :, 512:768] = plus(res_in[:, 512:768], rx[1, 0], rx[1, 1], rx[1, 2], rx[1, 3])
    with scope("drain"):
        for sent in families:
            all_of(sent).wait_send()
    assert len(families) <= N_SEND and len(groups) <= N_RECV, (len(families), len(groups))
    assert max(g.tiles for g in families + groups) <= N_TILES


def exchange(part, tokens, mid_gain, ids, weights, blend, eg, eu, ed, dg, du, dd):
    vm = pl.BlockSpec(memory_space=VMEM)
    hbm = pl.BlockSpec(memory_space=pl.ANY)
    return pl.pallas_call(
        exchange_kernel,
        name="exchange",
        out_shape=jax.ShapeDtypeStruct((2, ROWS, D // 2), BF16),
        in_specs=[vm] * 6 + [hbm] * 6,
        out_specs=vm,
        scratch_shapes=[
            VMEM((NX, NY, NZ, ROWS, WIDE), BF16),
            VMEM((NX, NY, NZ, ROWS, D), BF16),
            VMEM((2, 512, D), BF16),
            VMEM((2, 256, D), BF16),
            VMEM((2, ROWS, 128), F32),
            VMEM((ROWS, D), BF16), VMEM((2, ROWS, D // 2), BF16), VMEM((ROWS, D // 2), BF16),
            VMEM((4, 2, 4, ROWS, W), BF16), VMEM((4, 2, NZ, ROWS, W), BF16),
            VMEM((2, 4, ROWS, W), BF16), VMEM((2, NZ, ROWS, W), BF16),
            VMEM((2, 4, ROWS, W), BF16), VMEM((2, NZ, ROWS, W), BF16),
            VMEM((4, 2, 4, ROWS, W), BF16), VMEM((4, 2, NZ, ROWS, W), BF16),
            VMEM((4, NZ, ROWS, W), BF16), VMEM((4, NZ, ROWS, W), BF16),
            VMEM((2, NZ, ROWS, W), BF16), VMEM((2, NZ, ROWS, W), BF16),
            VMEM((2, 4, 4, NX, ROWS, W), BF16), VMEM((4, NX, ROWS, W), BF16),
            VMEM((4, NX, ROWS, W), BF16), VMEM((2, NX, ROWS, W // 2), BF16),
            VMEM((2, NX, ROWS, W // 2), BF16),
            VMEM((N_TILES, ROWS, 128), BF16),
            pltpu.SemaphoreType.DMA((N_SEND,)),
            pltpu.SemaphoreType.DMA((N_RECV,)),
            pltpu.SemaphoreType.DMA((16,)),
        ],
        compiler_params=pltpu.CompilerParams(collective_id=0, has_side_effects=True),
    )(part, tokens, mid_gain, ids, weights, blend, eg, eu, ed, dg, du, dd)


def shards(
    tokens, prior_state, first_gain, query_weight, key_weight, value_weight, decay_down, decay_up,
    decay_base, rate_down, rate_up, rate_base, head_gain, out_weight, mid_gain, route_ids,
    route_weights, expert_gate, expert_up, expert_down, dense_gate, dense_up, dense_down,
    blend_vector,
):
    part, new_state = mixer(
        tokens, prior_state, first_gain, query_weight, key_weight, value_weight, decay_down,
        decay_up, decay_base, rate_down, rate_up, rate_base, head_gain, out_weight,
    )
    mixed = exchange(
        part, tokens.reshape(2, ROWS, D), mid_gain.reshape(-1, 128), route_ids.T, route_weights.T,
        blend_vector, jnp.swapaxes(expert_gate, 1, 2),
        jnp.swapaxes(expert_up, 1, 2), expert_down, dense_gate.T, dense_up.T, dense_down,
    )
    return (mixed.reshape(2 * ROWS, D // 2), new_state)


def solution(mesh):
    split = Mesh(mesh.devices.reshape(NZ, NY, NX, mesh.shape["tp"]), EP_TP)
    in_specs = (
        P(EP, None),
        P(EP, "tp", None, None),
        P(),
        P(None, "tp"),
        P(None, "tp"),
        P(None, "tp"),
        P(),
        P(None, "tp"),
        P("tp"),
        P(),
        P(None, "tp"),
        P("tp"),
        P("tp"),
        P("tp", None),
        P(),
        P(EP, None),
        P(EP, None),
        P(EP, None, "tp"),
        P(EP, None, "tp"),
        P(EP, "tp", None),
        P(None, EP_TP),
        P(None, EP_TP),
        P(EP_TP, None),
        P(),
    )
    out_specs = (P(EP, "tp"), P(EP, "tp", None, None))
    return jax.shard_map(
        shards, mesh=split, in_specs=in_specs, out_specs=out_specs, check_vma=False
    )
```

```python
import math

import jax
import jax.numpy as jnp
from jax import lax
from jax.experimental import pallas as pl
from jax.experimental.pallas import tpu as pltpu
from jax.sharding import Mesh
from jax.sharding import PartitionSpec as P

EP = ("ep_0", "ep_1", "ep_2")
EP_TP = ("ep_0", "ep_1", "ep_2", "tp")
NZ, NY, NX = 8, 4, 4
F32 = jnp.float32
BF16 = jnp.bfloat16
MESH_ID = pl.DeviceIdType.MESH
VMEM = pltpu.VMEM

D = 1536
ROWS = 8
WIDE = D + 128
AGA = slice(0, 512)
AGB = slice(512, 1024)
AGAB = slice(0, 1024)
AGC = slice(1024, WIDE)
AGC_D = slice(1024, D)
CA = slice(0, 512)
CB = slice(512, 1024)
CC = slice(1024, 1536)
W = 512
N_SEND, N_RECV, N_TILES = 10, 160, 1152


def dot(a, b):
    return jnp.dot(a, b, preferred_element_type=F32)


def dot_t(a, b):
    return lax.dot_general(a, b, (((1,), (1,)), ((), ())), preferred_element_type=F32)


def flat(ref):
    return jnp.concatenate([ref[j : j + 1, :] for j in range(ref.shape[0])], axis=1)


scope = jax.named_scope


def mixer_kernel(
    tok_h, gain_h, wq_h, wk_h, wv_h, dd_h, du_h, db_h, rd_h, ru_h, rb_h, hg_h, wo_h, st_h,
    part_out, st_out,
    tok, gain, dd, du, db, rd, ru, rb, hg, part, wq, wk, wv, wo, st, dec_s, left_s, right_s, val_s, both_s, wsem, isem, osem,
):
    heads = st_h.shape[1]
    rows = tok.shape[0]
    loads = [
        pltpu.make_async_copy(src, dst, wsem.at[i])
        for i, (src, dst) in enumerate(((wk_h, wk), (wv_h, wv), (wq_h, wq), (wo_h, wo)))
    ]
    small = [
        pltpu.make_async_copy(src, dst, wsem.at[4 + i])
        for i, (src, dst) in enumerate(
            (
                (tok_h, tok), (gain_h, gain), (dd_h, dd), (rd_h, rd), (du_h, du), (ru_h, ru), (db_h, db),
                (rb_h, rb), (hg_h, hg),
            )
        )
    ]
    for load in small:
        load.start()
    for load in loads[:3]:
        load.start()
    states = [pltpu.make_async_copy(st_h.at[:, h], st.at[h], isem.at[h]) for h in range(heads)]
    for copy in states:
        copy.start()
    loads[3].start()
    with scope("m_norm"):
        for load in small:
            load.wait()
        token_f = tok[...].astype(F32)
        scale = lax.rsqrt(jnp.mean(token_f * token_f, axis=-1, keepdims=True) + 1e-06)
        normed = (token_f * scale * flat(gain)).astype(BF16)
        decay_low = jnp.tanh(dot_t(normed, dd[...])).astype(BF16)
        decay_in = flat(db) + dot(decay_low, du[...])
        decay = jnp.exp(-0.6065306597126334 * jax.nn.sigmoid(decay_in))
        rate_low = dot_t(normed, rd[...]).astype(BF16)
        learn = jax.nn.sigmoid(flat(rb) + dot(rate_low, ru[...]))
    with scope("m_qkv"):
        loads[0].wait()
        key = dot(normed, wk[...]).astype(BF16).astype(F32)
        loads[1].wait()
        value = dot(normed, wv[...]).astype(BF16).astype(F32)
        loads[2].wait()
        rec = dot(normed, wq[...]).astype(BF16).astype(F32)
    with scope("m_prep"):
        val_s[...] = jnp.transpose(jnp.concatenate([jnp.zeros_like(value), value], axis=0)).reshape(
            heads, 64, 2 * rows
        )
        taken, given = [], []
        for h in range(heads):
            lanes = slice(64 * h, 64 * h + 64)
            k, r, d = key[:, lanes], rec[:, lanes], decay[:, lanes]
            unit = k * lax.rsqrt(jnp.sum(k * k, axis=-1, keepdims=True) + 1e-06)
            rate = unit * learn[:, lanes]
            dec_s[h] = d
            left_s[h, 0:rows] = unit.astype(BF16)
            left_s[h, rows : 2 * rows] = (d * r).astype(BF16)
            right_s[h, 0:rows] = rate.astype(BF16)
            right_s[h, rows : 2 * rows] = k.astype(BF16)
            taken.append(jnp.sum(rate * r, axis=-1, keepdims=True))
            given.append(jnp.sum(k * r, axis=-1, keepdims=True))

    lane = lax.broadcasted_iota(jnp.int32, (64, 2 * rows), 1)

    def head(h, carry):
        pltpu.make_async_copy(st_h.at[:, h], st.at[h], isem.at[h]).wait()
        prior = st[h].reshape(rows * 64, 64)
        products = dot_t(prior.astype(BF16), left_s[h])
        own = jnp.zeros((64, 2 * rows), F32)
        values = val_s[h]
        outer = []
        for b in range(rows):
            here = products[64 * b : 64 * b + 64]
            first, second = lane == b, lane == rows + b
            own = jnp.where(first | second, here, own)
            outer.append(
                jnp.where(first, -here, jnp.where(second, values, 0.0)).astype(BF16)
            )
        change = dot(jnp.concatenate(outer, axis=0), right_s[h])
        for b in range(rows):
            part_b = slice(64 * b, 64 * b + 64)
            st[h, b] = prior[part_b] * dec_s[h, b : b + 1, :] + change[part_b]
        both_s[pl.ds(pl.multiple_of(h * 64, 64), 64), :] = own
        pltpu.make_async_copy(st.at[h], st_out.at[:, h], osem.at[h]).start()
        return carry

    with scope("m_state"):
        lax.fori_loop(0, heads, head, 0)
    with scope("m_out"):
        both = jnp.transpose(both_s[...])
        mixed = []
        for h in range(heads):
            lanes = slice(64 * h, 64 * h + 64)
            read = (
                both[rows : 2 * rows, lanes]
                - both[0:rows, lanes] * taken[h]
                + value[:, lanes] * given[h]
            )
            diff = read - jnp.mean(read, axis=-1, keepdims=True)
            spread = jnp.mean(diff * diff, axis=-1, keepdims=True)
            mixed.append(diff * lax.rsqrt(spread + 0.00064))
        mixed = (jnp.concatenate(mixed, axis=1) * flat(hg)).astype(BF16)
        loads[3].wait()
        partial = dot(mixed, wo[...])
        part[0] = partial[0:8].astype(BF16)
        part[1] = partial[8:16].astype(BF16)
        sent = pltpu.make_async_copy(part, part_out, wsem.at[4 + len(small)])
        sent.start()

    def drain(h, carry):
        pltpu.make_async_copy(st.at[h], st_out.at[:, h], osem.at[h]).wait()
        return carry

    with scope("m_drain"):
        lax.fori_loop(0, heads, drain, 0)
        sent.wait()


def mixer(tokens, prior_state, first_gain, wq, wk, wv, dd, du, db, rd, ru, rb, hg, wo):
    rows, heads = prior_state.shape[:2]
    hbm = pl.BlockSpec(memory_space=pl.ANY)
    inner = heads * 64
    return pl.pallas_call(
        mixer_kernel,
        name="mixer",
        out_shape=(
            jax.ShapeDtypeStruct((2, rows // 2, D), BF16),
            jax.ShapeDtypeStruct(prior_state.shape, F32),
        ),
        in_specs=[hbm] * 14,
        out_specs=(hbm, hbm),
        scratch_shapes=[
            VMEM((rows, D), BF16), VMEM((D // 128, 128), F32),
            VMEM(dd.shape[::-1], BF16), VMEM(du.shape, BF16), VMEM((inner // 128, 128), F32),
            VMEM(rd.shape[::-1], BF16), VMEM(ru.shape, BF16), VMEM((inner // 128, 128), F32),
            VMEM((inner // 128, 128), F32), VMEM((2, rows // 2, D), BF16),
            VMEM((D, inner), BF16), VMEM((D, inner), BF16), VMEM((D, inner), BF16),
            VMEM((inner, D), BF16), VMEM((heads, rows, 64, 64), F32),
            VMEM((heads, rows, 64), F32),
            VMEM((heads, 2 * rows, 64), BF16), VMEM((heads, 2 * rows, 64), BF16),
            VMEM((heads, 64, 2 * rows), F32), VMEM((inner, 2 * rows), F32),
            pltpu.SemaphoreType.DMA((14,)),
            pltpu.SemaphoreType.DMA((heads,)),
            pltpu.SemaphoreType.DMA((heads,)),
        ],
    )(
        tokens, first_gain.reshape(-1, 128), wq, wk, wv, dd.T, du, db.reshape(-1, 128), rd.T, ru,
        rb.reshape(-1, 128), hg.reshape(-1, 128), wo, prior_state,
    )


class Group:
    def __init__(self, index, copies=None):
        self.index, self.copies, self.tiles, self.sent = index, copies, 0, 0
        self.time, self.waited = 0.0, False


RATE = 46600.0
V1 = V2 = V3 = V3R = True
V4 = V4R = False
ORDER = (0, 1, 2, -1)
Z_ORDER = (4, 3, -3, 2, -2, 1, -1)
NEAR_RATE = 600000.0
START, HOP = 1.8, 0.85


class Plan:
    def __init__(self, arrive):
        self.arrive, self.now, self.links, self.steps = arrive, 0.0, {}, []

    def add(self, run, needs=(), after=(), cost=0.03, rank=5):
        step = dict(run=run, needs=needs, after=after, cost=cost, rank=rank, done=False, at=len(self.steps))
        self.steps.append(step)
        return step

    def sending(self, got, size, hops):
        begin = self.now
        end = begin + (0.0 if any(hops) else size / NEAR_RATE)
        for axis, hop in enumerate(hops):
            length = (NX, NY, NZ)[axis]
            ways = (1, -1) if 2 * abs(hop) == length else (1 if hop > 0 else -1,)
            for way in ways if hop else ():
                busy = max(begin, self.links.get((axis, way), 0.0)) + size * abs(hop) / len(ways) / RATE
                self.links[axis, way] = busy
                end = max(end, busy)
        got.sent += 1
        got.time = max(got.time, end + START + HOP * sum(abs(hop) for hop in hops))

    def run(self):
        waiting = list(self.steps)
        while waiting:
            open_ = [
                t for t in waiting
                if all(u["done"] for u in t["after"])
                and all(g.sent == g.copies for g in t["needs"])
            ]

            def when(t):
                return max([self.now] + [g.time for g in t["needs"] if not g.waited])

            step = min(open_, key=lambda t: (when(t), t["rank"], t["at"]))
            self.now = when(step) + step["cost"]
            for g in step["needs"]:
                if not g.waited:
                    self.arrive(g)
                    g.waited = True
            step["run"]()
            step["done"], step["end"] = True, self.now
            waiting.remove(step)


AROUND = (2, 1, -1, 0)
UP4, DOWN4 = (2, 1), (-1, 0)


def exchange_kernel(
    part_h, tok_h, gain_h, ids_h, weights_h, blend_h, eg_h, eu_h, ed_h, dg_h, du_h, dd_h,
    out,
    part, tok, gain, ids, weights, blend, full, made, w1, w2, shares_s, sums_s, peer_part, res_s, res_in,
    ax1, axf, ay1, ayf, bx1, bxf, by1, byf, a2, b2, z3, r3, cz, c2, ry, c3, rx, ry_a, rx_b, rxy, c4, czn, czf, tiles,
    send_sem, recv_sem, load_sem,
):
    z, y, x = (lax.axis_index(a) for a in EP)
    c = lax.axis_index("tp")
    expert = (z * NY + y) * NX + x
    families, groups = [], []

    def xa(d):
        return lax.rem(x + d + NX, NX)

    def ya(d):
        return lax.rem(y + d + NY, NY)

    def za(d):
        return lax.rem(z + d + NZ, NZ)

    def dev(dx=0, dy=0, dz=0, dc=0):
        return {
            "ep_0": za(dz) if dz else z,
            "ep_1": ya(dy) if dy else y,
            "ep_2": xa(dx) if dx else x,
            "tp": 1 - c if dc else c,
        }

    def family():
        families.append(Group(len(families)))
        return families[-1]

    def group(copies=1):
        return Group(None, copies)

    def send(src, dst, place, sent, got):
        if got.index is None:
            got.index = len(groups)
            groups.append(got)
        size = math.prod(src.shape) // (ROWS * 128)
        sent.tiles += size
        got.tiles += size
        place = dict(place)
        plan.sending(got, size * 2048, [place.get(k, 0) for k in ("dx", "dy", "dz")])
        to = dev(**place)
        pltpu.make_async_remote_copy(
            src_ref=src, dst_ref=dst, send_sem=send_sem.at[sent.index],
            recv_sem=recv_sem.at[got.index], device_id=to, device_id_type=MESH_ID,
        ).start()
        return got

    def all_of(g):
        view = tiles.at[pl.ds(0, g.tiles)]
        return pltpu.make_async_remote_copy(
            src_ref=view, dst_ref=view,
            send_sem=send_sem.at[g.index if g in families else 0],
            recv_sem=recv_sem.at[g.index if g in groups else 0],
            device_id=dev(dc=1), device_id_type=MESH_ID,
        )

    def arrive(*some):
        for g in some:
            assert g.sent == g.copies
            all_of(g).wait_recv()

    plan = Plan(arrive)

    first = [
        pltpu.make_async_copy(src, dst, load_sem.at[16 + i])
        for i, (src, dst) in enumerate(
            (
                (ids_h, ids), (weights_h, weights), (blend_h, blend), (part_h, part), (tok_h, tok), (gain_h, gain),
            )
        )
    ]
    for load in first:
        load.start()
    pieces = [
        (eg_h.at[0], w1.at[0, pl.ds(0, 192), :]),
        (dg_h, w1.at[0, pl.ds(192, 24), :]),
        (eu_h.at[0], w1.at[0, pl.ds(256, 192), :]),
        (du_h, w1.at[0, pl.ds(448, 24), :]),
    ]
    for k, at in enumerate((0, 768, 256, 1024, 512, 1280)):
        here, there = pl.ds(256 * k, 256), pl.ds(at, 256)
        pieces.append((ed_h.at[0, :, there], w2.at[0, pl.ds(0, 192), here]))
        pieces.append((dd_h.at[:, there], w2.at[0, pl.ds(192, 24), here]))
    loads = [pltpu.make_async_copy(src, dst, load_sem.at[i]) for i, (src, dst) in enumerate(pieces)]
    for load in loads:
        load.start()

    with scope("barrier"):
        peers = (
            [
                dev(dx=d, dy=f, dc=e)
                for d in range(NX) for f in range(NY) for e in (0, 1)
                if d or f or e
            ]
            + [dev(dz=d, dc=e) for d in range(1, NZ) for e in (0, 1)]
        )
        barrier = pltpu.get_barrier_semaphore()
        for peer in peers:
            pl.semaphore_signal(barrier, inc=1, device_id=peer, device_id_type=MESH_ID)
    with scope("shares"):
        for load in first:
            load.wait()
        own_w = weights[...]
        share = own_w / jnp.sum(own_w, axis=0, keepdims=True) * 2.5
        sub = lax.broadcasted_iota(jnp.int32, (128, 2 * ROWS), 0)
        shares = jnp.zeros((128, 2 * ROWS), F32)
        for k in range(own_w.shape[0]):
            shares = shares + jnp.where(ids[k : k + 1, :] == sub, share[k : k + 1, :], 0.0)
        shares_s[...] = jnp.transpose(shares).reshape(2, ROWS, 128)
        full[x, y, z, :, D:WIDE] = shares_s[c].astype(BF16)
        first_row = lax.broadcasted_iota(jnp.int32, (ROWS, D), 0) == 0
        w1[0, 216:224, :] = jnp.where(first_row, blend[...].astype(F32).reshape(1, D), 0.0).astype(BF16)
        w1[0, 224:256, :] = jnp.zeros((32, D), BF16)
        w1[0, 472:512, :] = jnp.zeros((40, D), BF16)
        w2[0, 216:256, :] = jnp.zeros((40, D), BF16)

    with scope("wait_all"):
        pl.semaphore_wait(barrier, len(peers))
    near = family()
    swap = send(part.at[1 - c], peer_part, dict(dc=1), near, group())

    with scope("mid"):
        arrive(swap)
        attn = part[c].astype(F32) + peer_part[...].astype(F32)
        resid_bf = (tok[c].astype(F32) + attn).astype(BF16)
        resid = resid_bf.astype(F32)
        scale = lax.rsqrt(jnp.mean(resid * resid, axis=-1, keepdims=True) + 1e-06)
        full[x, y, z, :, 0:D] = (resid * scale * flat(gain)).astype(BF16)
        res_s[0] = resid_bf[:, 0:768]
        res_s[1] = resid_bf[:, 768:1536]

    yp, ym, xp, xm = dict(dy=1), dict(dy=-1), dict(dx=1), dict(dx=-1)
    zp, zm = dict(dz=1), dict(dz=-1)
    fam_z, fam_a, fam_b, fam_c = family(), family(), family(), family()

    zab = group(7)
    for d in Z_ORDER:
        ref = full.at[x, y, z, :, AGAB]
        send(ref, ref, dict(dz=d), fam_z, zab)
    cx = group(3)
    cxy = {q: group(4 if q else 3) for q in AROUND}
    ref = full.at[x, y, z, :, AGC]
    if V3:
        for d in AROUND:
            for q in (2, 1, -1, 0):
                if d or q:
                    send(ref, ref, dict(dx=d, dy=q), fam_z, cxy[-q if q != 2 else 2])
    else:
        for d in (2, 1, -1):
            send(ref, ref, dict(dx=d), fam_z, cx)

    resid_in = group()
    send(res_s.at[1 - c], res_in, dict(dc=1), near, resid_in)
    with scope("w_load"):
        for load in loads:
            load.wait()
    w_fam, w_in = family(), group(2)
    send(w1.at[0], w1.at[1], dict(dc=1), w_fam, w_in)
    send(w2.at[0], w2.at[1], dict(dc=1), w_fam, w_in)

    def halves_out(ref_of, up, down, fam, first, rest):
        for at, half, to in ((0, 0, up), (1, 1, down), (0, 1, up), (1, 0, down)):
            ref = ref_of(0, half)
            send(ref, ref, to, fam, first[at] if half == at else rest[at])

    def halves_on(ref_of, up, down, fam, first, last):
        def on(at, d, to):
            def run():
                ref = ref_of(d, at)
                send(ref, ref, to, fam, last)

            return run

        return [
            plan.add(on(at, d, to), needs=[first[at]], after=[], rank=2)
            for at, d, to in ((0, -1, up), (1, 1, down))
        ]

    def a_y(d, half):
        return full.at[x, ya(d), pl.ds(4 * half, 4), :, AGA]

    def b_x(d, half):
        return full.at[xa(d), y, pl.ds(4 * half, 4), :, AGB]

    def a_x(j):
        return lambda d, half: full.at[xa(d), ya(j), pl.ds(4 * half, 4), :, AGA]

    def b_y(i):
        return lambda d, half: full.at[xa(i), ya(d), pl.ds(4 * half, 4), :, AGB]

    ay_first, ay_rest, ay_last = (group(), group()), (group(), group()), group(2)
    bx_first, bx_rest, bx_last = (group(), group()), (group(), group()), group(2)
    ax_first = {j: (group(), group()) for j in AROUND}
    by_first = {i: (group(), group()) for i in AROUND}
    ax_rest = {j: group(2) for j in AROUND}
    ax_last = {j: group(2) for j in AROUND}
    by_rest, by_last = (group(4), group(4)), group(8)

    def first_out():
        halves_out(a_y, yp, ym, fam_a, ay_first, ay_rest)
        halves_out(b_x, xp, xm, fam_b, bx_first, bx_rest)

    def a_out(j):
        return lambda: halves_out(a_x(j), xp, xm, fam_a, ax_first[j], (ax_rest[j], ax_rest[j]))

    def b_out(i):
        return lambda: halves_out(b_y(i), yp, ym, fam_b, by_first[i], by_rest)

    ay_in = {j: group() for j in (1, -1, 2)}
    bx_in = {j: group() for j in (1, -1, 2)}

    def direct_out():
        ref = full.at[x, y, :, :, AGA]
        for d in (2, 1, -1):
            send(ref, ref, dict(dy=d), fam_a, ay_in[d])
        ref = full.at[x, y, :, :, AGB]
        for d in (2, 1, -1):
            send(ref, ref, dict(dx=d), fam_b, bx_in[d])

    if V1:
        plan.add(direct_out, needs=[zab], rank=0)
    else:
        plan.add(first_out, needs=[zab], rank=0)
        halves_on(a_y, yp, ym, fam_a, ay_first, ay_last)
        halves_on(b_x, xp, xm, fam_b, bx_first, bx_last)
    for j, at in ((0, None), (1, 1), (-1, 0), (2, 2)):
        a_needs = [zab] if at is None else [ay_last] if at == 2 else [ay_first[at], ay_rest[at]]
        b_needs = [zab] if at is None else [bx_last] if at == 2 else [bx_first[at], bx_rest[at]]
        if V1 and j:
            a_needs, b_needs = [ay_in[-j if j != 2 else 2]], [bx_in[-j if j != 2 else 2]]
        plan.add(a_out(j), needs=a_needs, rank=3)
        plan.add(b_out(j), needs=b_needs, rank=3)
        halves_on(a_x(j), xp, xm, fam_a, ax_first[j], ax_last[j])
        halves_on(b_y(j), yp, ym, fam_b, by_first[j], by_last)

    up_in = {(t, q): group() for t in (1, 2, 3) for q in AROUND}
    down_in = {(t, q): group() for t in (1, 2, 3) for q in AROUND}
    c_last = {q: group() for q in AROUND}

    two_in = {(q, up): group() for q in AROUND for up in (True, False)}
    z_rest = {q: group(5) for q in AROUND}

    def c_near(q, up):
        def run():
            ref = full.at[:, ya(q), z, :, AGC]
            send(ref, ref, dict(dz=2 if up else -2), fam_c, two_in[q, up])
            send(ref, ref, dict(dz=1 if up else -1), fam_c, z_rest[q])

        return run

    def c_far(q, up):
        def run():
            ref = full.at[:, ya(q), za(-2 if up else 2), :, AGC]
            if q in (UP4 if up else DOWN4):
                send(ref, ref, dict(dz=2 if up else -2), fam_c, z_rest[q])
            send(ref, ref, dict(dz=1 if up else -1), fam_c, z_rest[q])

        return run

    def c_z(t, q, up):
        def run():
            ref = full.at[:, ya(q), za(1 - t if up else t - 1), :, AGC]
            got = c_last[q] if t == 4 else (up_in if up else down_in)[t, q]
            send(ref, ref, zp if up else zm, fam_c, got)

        return run

    cy = {1: group(2), 2: group()}

    def c_out():
        for d in (2, 1, -1):
            ref = full.at[:, y, z, :, AGC]
            send(ref, ref, dict(dy=d), fam_c, cy[abs(d)])

    if not V3:
        plan.add(c_out, needs=[cx], rank=0)
    for q in (0, 1, -1, 2):
        for up in (True, False):
            c_needs = [cxy[q]] if V3 else [cy[abs(q)] if q else cx]
            if V4:
                plan.add(c_near(q, up), needs=c_needs, rank=1)
                plan.add(c_far(q, up), needs=[two_in[q, up]], rank=1)
                continue
            plan.add(c_z(1, q, up), needs=c_needs, rank=1)
            got = up_in if up else down_in
            for t in (2, 3, 4):
                if t < 4 or q in (UP4 if up else DOWN4):
                    plan.add(c_z(t, q, up), needs=[got[t - 1, q]], rank=1)

    slot = {j: k for k, j in enumerate(AROUND)}
    lane128 = lax.broadcasted_iota(jnp.int32, (256, 128), 1)
    lane256 = lax.broadcasted_iota(jnp.int32, (256, 256), 1)

    begun = set()

    def part_of(j, cols):
        def run():
            mid = full[:, ya(j), :, :, cols].reshape(256, cols.stop - cols.start)
            for half in range(2):
                term = dot_t(mid, w1[half, :, cols])
                sums_s[slot[j], half] = sums_s[slot[j], half] + term if j in begun else term
            begun.add(j)

        return run

    def made_of(j):
        def run():
            chosen = full[:, ya(j), :, :, D:WIDE].reshape(256, 128).astype(F32)
            chosen = jnp.sum(jnp.where(lane128 == expert, chosen, 0.0), axis=1, keepdims=True)
            level = jnp.where(lane256 < 192, chosen, jax.nn.sigmoid(sums_s[slot[j], 0, :, 216:217]))
            total = None
            for half in range(2):
                g, u = sums_s[slot[j], half, :, 0:256], sums_s[slot[j], half, :, 256:512]
                hidden = (g * jax.nn.sigmoid(g) * u * level).astype(BF16)
                term = dot(hidden, w2[half])
                total = term if total is None else total + term
            made[:, ya(j)] = total.astype(BF16).reshape(NX, NZ, ROWS, D)

        return run

    every = lambda q: [two_in[q, True], two_in[q, False], z_rest[q]] if V4 else [up_in[t, q] for t in (1, 2, 3)] + [down_in[t, q] for t in (1, 2, 3)] + [c_last[q]]
    row_needs = {
        0: list(bx_in.values()) if V1 else [*bx_first, *bx_rest, bx_last],
        1: [by_rest[1]] + [by_first[i][1] for i in AROUND],
        -1: [by_rest[0]] + [by_first[i][0] for i in AROUND],
        2: [by_last],
    }
    layer = {}
    for rank, j in enumerate(ORDER):
        a_part = plan.add(
            part_of(j, AGA), needs=[w_in, *ax_first[j], ax_rest[j], ax_last[j]],
            cost=0.37, rank=20 + rank,
        )
        b_part = plan.add(part_of(j, AGB), needs=[w_in, *row_needs[j]], cost=0.37, rank=20 + rank)
        c_part = plan.add(part_of(j, AGC_D), needs=[w_in, *every(j)], cost=0.37, rank=20 + rank)
        layer[j] = plan.add(
            made_of(j), needs=every(j), after=[a_part, b_part, c_part], cost=0.65, rank=10 + rank
        )

    def plus(*terms):
        total = terms[0].astype(F32)
        for term in terms[1:]:
            total = total + term.astype(F32)
        return total.astype(BF16)

    lower, upper = pl.ds(0, 4), pl.ds(4, 4)
    rs_a, rs_b, rs_c, rs_z = family(), family(), family(), family()
    ax_one = {j: (group(), group()) for j in AROUND}
    ax_fin = {j: group(4) for j in AROUND}
    by_one = {i: (group(), group()) for i in AROUND}
    by_fin = {i: group(4) for i in AROUND}

    def a_start(j):
        def run():
            k, yj = slot[j], ya(j)
            send(made.at[xa(2), yj, lower, :, CA], ax1.at[k, 0], xp, rs_a, ax_one[j][0])
            send(made.at[xa(2), yj, upper, :, CA], ax1.at[k, 1], xm, rs_a, ax_one[j][1])
            send(made.at[xa(1), yj, upper, :, CA], axf.at[k, 0, upper], xp, rs_a, ax_fin[j])
            send(made.at[xa(-1), yj, lower, :, CA], axf.at[k, 1, lower], xm, rs_a, ax_fin[j])

        return run

    def a_on(j, at):
        def run():
            k, yj = slot[j], ya(j)
            if at == 0:
                made[xa(1), yj, 0:4, :, CA] = plus(made[xa(1), yj, 0:4, :, CA], ax1[k, 0])
                send(made.at[xa(1), yj, lower, :, CA], axf.at[k, 0, lower], xp, rs_a, ax_fin[j])
            else:
                made[xa(-1), yj, 4:8, :, CA] = plus(made[xa(-1), yj, 4:8, :, CA], ax1[k, 1])
                send(made.at[xa(-1), yj, upper, :, CA], axf.at[k, 1, upper], xm, rs_a, ax_fin[j])

        return run

    def a_end(j):
        return plus(made[x, ya(j), :, :, CA], axf[slot[j], 0], axf[slot[j], 1])

    def b_start(i):
        def run():
            k, xi = slot[i], xa(i)
            send(made.at[xi, ya(2), lower, :, CB], by1.at[k, 0], yp, rs_b, by_one[i][0])
            send(made.at[xi, ya(2), upper, :, CB], by1.at[k, 1], ym, rs_b, by_one[i][1])

        return run

    def b_free(i, d):
        def run():
            k, xi = slot[i], xa(i)
            if d > 0:
                send(made.at[xi, ya(1), upper, :, CB], byf.at[k, 0, upper], yp, rs_b, by_fin[i])
            else:
                send(made.at[xi, ya(-1), lower, :, CB], byf.at[k, 1, lower], ym, rs_b, by_fin[i])

        return run

    def b_on(i, at):
        def run():
            k, xi = slot[i], xa(i)
            if at == 0:
                made[xi, ya(1), 0:4, :, CB] = plus(made[xi, ya(1), 0:4, :, CB], by1[k, 0])
                send(made.at[xi, ya(1), lower, :, CB], byf.at[k, 0, lower], yp, rs_b, by_fin[i])
            else:
                made[xi, ya(-1), 4:8, :, CB] = plus(made[xi, ya(-1), 4:8, :, CB], by1[k, 1])
                send(made.at[xi, ya(-1), upper, :, CB], byf.at[k, 1, upper], ym, rs_b, by_fin[i])

        return run

    def b_end(i):
        return plus(made[xa(i), y, :, :, CB], byf[slot[i], 0], byf[slot[i], 1])

    def second(blocks, buf, one, fin, up, down, fam, all_in):
        got, end = (group(), group()), group(4)
        put = {}
        for j in AROUND:
            block, needs, after = blocks(j)

            def run(j=j, block=block):
                k = slot[j]
                buf[k] = block(j)
                if V2:
                    if j:
                        send(buf.at[k], all_in.at[k], dict(zip(("dy" if "dy" in up else "dx",), (j,))), fam, end)
                elif j == 2:
                    send(buf.at[k, lower], one.at[0], up, fam, got[0])
                    send(buf.at[k, upper], one.at[1], down, fam, got[1])
                elif j == 1:
                    send(buf.at[k, upper], fin.at[0, upper], up, fam, end)
                elif j == -1:
                    send(buf.at[k, lower], fin.at[1, lower], down, fam, end)

            put[j] = plan.add(run, needs=needs, after=after, cost=0.1, rank=3)
        if V2:
            end.copies = 3
            return end, put[0]

        def on_up():
            k = slot[1]
            buf[k, 0:4] = plus(buf[k, 0:4], one[0])
            send(buf.at[k, lower], fin.at[0, lower], up, fam, end)

        def on_down():
            k = slot[-1]
            buf[k, 4:8] = plus(buf[k, 4:8], one[1])
            send(buf.at[k, upper], fin.at[1, upper], down, fam, end)

        plan.add(on_up, needs=[got[0]], after=[put[1]], cost=0.06, rank=2)
        plan.add(on_down, needs=[got[1]], after=[put[-1]], cost=0.06, rank=2)
        return end, put[0]

    c_up = {(t, q): group() for t in (1, 2, 3) for q in AROUND if t > 1 or q in UP4}
    c_down = {(t, q): group() for t in (1, 2, 3) for q in AROUND if t > 1 or q in DOWN4}
    c_fin = {q: group(4 if V4R else 2) for q in AROUND}

    def c_send(t, q, up):
        way, to = (0, zp) if up else (1, zm)
        at = za(5 - t) if up else za(t - 5)
        got = c_fin[q] if t == 4 else (c_up if up else c_down)[t, q]
        send(made.at[:, ya(q), at, :, CC], cz.at[way, t - 1, slot[q]], to, rs_c, got)

    def c_start(q):
        def run():
            c_send(1, q, q in UP4)
            c_send(2, q, q in DOWN4)

        return run

    c_three = {(q, up): group(2 if q in (UP4 if up else DOWN4) else 1) for q in AROUND for up in (True, False)}

    def c_first(q):
        def run():
            k = slot[q]
            for up in (True, False):
                way, sign = (0, 1) if up else (1, -1)
                if q in (UP4 if up else DOWN4):
                    send(made.at[:, ya(q), za(4), :, CC], czf.at[way, 1, k], dict(dz=2 * sign), rs_c, c_three[q, up])
                send(made.at[:, ya(q), za(3 * sign), :, CC], czf.at[way, 0, k], dict(dz=sign), rs_c, c_three[q, up])
                send(made.at[:, ya(q), za(sign), :, CC], czn.at[way, k], dict(dz=sign), rs_c, c_fin[q])

        return run

    def c_sum(q, up):
        def run():
            k = slot[q]
            way, sign = (0, 1) if up else (1, -1)
            at = za(2 * sign)
            terms = [made[:, ya(q), at, :, CC], czf[way, 0, k]]
            if q in (UP4 if up else DOWN4):
                terms.append(czf[way, 1, k])
            made[:, ya(q), at, :, CC] = plus(*terms)
            send(made.at[:, ya(q), at, :, CC], czn.at[2 + way, k], dict(dz=2 * sign), rs_c, c_fin[q])

        return run

    def c_on(t, q, up):
        def run():
            at = za(5 - t) if up else za(t - 5)
            made[:, ya(q), at, :, CC] = plus(
                made[:, ya(q), at, :, CC], cz[0 if up else 1, t - 2, slot[q]]
            )
            c_send(t, q, up)

        return run

    cy_in = group(3)
    xy_same, xy_other = group(15), group(16)

    def c_end(q):
        def run():
            k = slot[q]
            if V4R:
                sums = plus(made[:, ya(q), z, :, CC], czn[0, k], czn[1, k], czn[2, k], czn[3, k])
            else:
                sums = plus(made[:, ya(q), z, :, CC], cz[0, 3, k], cz[1, 3, k])
            if V3R:
                c4[k, 0] = sums[:, :, 0:256]
                c4[k, 1] = sums[:, :, 256:512]
                for d in AROUND:
                    i = (d + NX) % NX
                    send(c4.at[k, 1 - c, xa(d)], rxy.at[1, k, i], dict(dx=d, dy=q, dc=1), rs_z, xy_other)
                    if d or q:
                        send(c4.at[k, c, xa(d)], rxy.at[0, k, i], dict(dx=d, dy=q), rs_z, xy_same)
                return
            c2[k] = sums
            if q:
                send(c2.at[k], ry.at[k], dict(dy=q), rs_c, cy_in)

        return run

    c_ends = []
    for j in AROUND:
        if V4R:
            begun = plan.add(c_first(j), after=[layer[j]], rank=0)
            for up in (True, False):
                plan.add(c_sum(j, up), needs=[c_three[j, up]], after=[begun], cost=0.08, rank=1)
        else:
            plan.add(c_start(j), after=[layer[j]], rank=0)
        a_begun = plan.add(a_start(j), after=[layer[j]], rank=1)
        for at in (0, 1):
            plan.add(a_on(j, at), needs=[ax_one[j][at]], after=[a_begun], cost=0.06, rank=2)
        for up, got in ((True, c_up), (False, c_down)):
            for t in () if V4R else (2, 3, 4):
                if (t - 1, j) in got:
                    plan.add(c_on(t, j, up), needs=[got[t - 1, j]], after=[layer[j]], cost=0.06, rank=1)
        c_ends.append(plan.add(c_end(j), needs=[c_fin[j]], after=[layer[j]], cost=0.08, rank=1))
        plan.add(b_start(j), after=[layer[2]], rank=1)
        for d in (1, -1):
            plan.add(b_free(j, d), after=[layer[d]], rank=4)
            plan.add(b_on(j, 0 if d > 0 else 1), needs=[by_one[j][0 if d > 0 else 1]], after=[layer[d]], cost=0.06, rank=2)

    a_sum, a_own = second(lambda j: (a_end, [ax_fin[j]], [layer[j]]), a2, ay1, ayf, yp, ym, rs_a, ry_a)
    b_sum, b_own = second(lambda j: (b_end, [by_fin[j]], [layer[0]]), b2, bx1, bxf, xp, xm, rs_b, rx_b)
    z_same, z_other, x_in = group(7), group(8), group(7)

    za_same, za_other, zb_same, zb_other = group(7), group(8), group(7), group(8)

    def z_out(buf, into, at, same, other):
        def run():
            sums = plus(buf[3], into[0], into[1], into[2])
            z3[0, :, :, at : at + 256] = sums[:, :, 0:256]
            z3[1, :, :, at : at + 256] = sums[:, :, 256:512]
            here = pl.ds(at, 256)
            for d in (4, 3, -3, 2, -2, 1, -1, 0):
                k = (d + NZ) % NZ
                send(z3.at[1 - c, za(d), :, here], r3.at[1, k, :, here], dict(dz=d, dc=1), rs_z, other)
                if d:
                    send(z3.at[c, za(d), :, here], r3.at[0, k, :, here], dict(dz=d), rs_z, same)

        return run

    def c_out_x():
        sums_c = plus(*(ry[slot[q]] for q in (1, -1, 2)), c2[slot[0]])
        c3[0] = sums_c[:, :, 0:256]
        c3[1] = sums_c[:, :, 256:512]
        for d in (2, 1, -1, 0):
            k = (d + NX) % NX
            send(c3.at[1 - c, xa(d)], rx.at[1, k], dict(dx=d, dc=1), rs_z, x_in)
            if d:
                send(c3.at[c, xa(d)], rx.at[0, k], dict(dx=d), rs_z, x_in)

    def out_z(at):
        def run():
            cols = slice(at, at + 256)
            total = res_s[c, :, cols].astype(F32) + z3[c, z, :, cols].astype(F32)
            for d in range(1, NZ):
                total = total + r3[0, d, :, cols].astype(F32)
            out[c, :, cols] = total.astype(BF16)
            total = res_in[:, cols].astype(F32)
            for d in range(NZ):
                total = total + r3[1, d, :, cols].astype(F32)
            out[1 - c, :, cols] = total.astype(BF16)

        return run

    def out_c():
        out[c, :, 512:768] = plus(res_s[c, :, 512:768], c3[c, x], rx[0, 1], rx[0, 2], rx[0, 3])
        out[1 - c, :, 512:768] = plus(res_in[:, 512:768], rx[1, 0], rx[1, 1], rx[1, 2], rx[1, 3])

    def out_c_same():
        total = res_s[c, :, 512:768].astype(F32)
        for k in range(NY):
            for i in range(NX):
                total = total + (c4[3, c, x] if k == 3 and i == 0 else rxy[0, k, i]).astype(F32)
        out[c, :, 512:768] = total.astype(BF16)

    def out_c_other():
        total = res_in[:, 512:768].astype(F32)
        for k in range(NY):
            for i in range(NX):
                total = total + rxy[1, k, i].astype(F32)
        out[1 - c, :, 512:768] = total.astype(BF16)

    a_sent = plan.add(z_out(a2, ry_a, 0, za_same, za_other), needs=[a_sum], after=[a_own], cost=0.12, rank=0)
    b_sent = plan.add(z_out(b2, rx_b, 256, zb_same, zb_other), needs=[b_sum], after=[b_own], cost=0.12, rank=0)
    if V3R:
        plan.add(out_c_same, needs=[resid_in, xy_same], after=c_ends, cost=0.1)
        plan.add(out_c_other, needs=[resid_in, xy_other], after=c_ends, cost=0.1)
    else:
        x_sent = plan.add(c_out_x, needs=[cy_in], after=c_ends, cost=0.1, rank=0)
        plan.add(out_c, needs=[resid_in, x_in], after=[x_sent], cost=0.1)
    plan.add(out_z(0), needs=[resid_in, za_same, za_other], after=[a_sent], cost=0.1)
    plan.add(out_z(256), needs=[resid_in, zb_same, zb_other], after=[b_sent], cost=0.1)
    plan.run()
    with scope("drain"):
        for sent in families:
            all_of(sent).wait_send()
    assert len(families) <= N_SEND and len(groups) <= N_RECV, (len(families), len(groups))
    assert max(g.tiles for g in families + groups) <= N_TILES


def exchange(part, tokens, mid_gain, ids, weights, blend, eg, eu, ed, dg, du, dd):
    vm = pl.BlockSpec(memory_space=VMEM)
    hbm = pl.BlockSpec(memory_space=pl.ANY)
    return pl.pallas_call(
        exchange_kernel,
        name="exchange",
        out_shape=jax.ShapeDtypeStruct((2, ROWS, D // 2), BF16),
        in_specs=[hbm] * 12,
        out_specs=vm,
        scratch_shapes=[
            VMEM((2, ROWS, D), BF16), VMEM((2, ROWS, D), BF16), VMEM((D // 128, 128), F32),
            VMEM(ids.shape, ids.dtype), VMEM(weights.shape, F32), VMEM((D,), BF16),
            VMEM((NX, NY, NZ, ROWS, WIDE), BF16),
            VMEM((NX, NY, NZ, ROWS, D), BF16),
            VMEM((2, 512, D), BF16),
            VMEM((2, 256, D), BF16),
            VMEM((2, ROWS, 128), F32),
            VMEM((4, 2, 256, 512), F32),
            VMEM((ROWS, D), BF16), VMEM((2, ROWS, D // 2), BF16), VMEM((ROWS, D // 2), BF16),
            VMEM((4, 2, 4, ROWS, W), BF16), VMEM((4, 2, NZ, ROWS, W), BF16),
            VMEM((2, 4, ROWS, W), BF16), VMEM((2, NZ, ROWS, W), BF16),
            VMEM((2, 4, ROWS, W), BF16), VMEM((2, NZ, ROWS, W), BF16),
            VMEM((4, 2, 4, ROWS, W), BF16), VMEM((4, 2, NZ, ROWS, W), BF16),
            VMEM((4, NZ, ROWS, W), BF16), VMEM((4, NZ, ROWS, W), BF16),
            VMEM((2, NZ, ROWS, W), BF16), VMEM((2, NZ, ROWS, W), BF16),
            VMEM((2, 4, 4, NX, ROWS, W), BF16), VMEM((4, NX, ROWS, W), BF16),
            VMEM((4, NX, ROWS, W), BF16), VMEM((2, NX, ROWS, W // 2), BF16),
            VMEM((2, NX, ROWS, W // 2), BF16),
            VMEM((3, NZ, ROWS, W), BF16), VMEM((3, NZ, ROWS, W), BF16),
            VMEM((2, NY, NX, ROWS, W // 2), BF16), VMEM((4, 2, NX, ROWS, W // 2), BF16),
            VMEM((4, 4, NX, ROWS, W), BF16), VMEM((2, 2, 4, NX, ROWS, W), BF16),
            VMEM((N_TILES, ROWS, 128), BF16),
            pltpu.SemaphoreType.DMA((N_SEND,)),
            pltpu.SemaphoreType.DMA((N_RECV,)),
            pltpu.SemaphoreType.DMA((22,)),
        ],
        compiler_params=pltpu.CompilerParams(collective_id=0, has_side_effects=True),
    )(part, tokens, mid_gain, ids, weights, blend, eg, eu, ed, dg, du, dd)


def shards(
    tokens, prior_state, first_gain, query_weight, key_weight, value_weight, decay_down, decay_up,
    decay_base, rate_down, rate_up, rate_base, head_gain, out_weight, mid_gain, route_ids,
    route_weights, expert_gate, expert_up, expert_down, dense_gate, dense_up, dense_down,
    blend_vector,
):
    part, new_state = mixer(
        tokens, prior_state, first_gain, query_weight, key_weight, value_weight, decay_down,
        decay_up, decay_base, rate_down, rate_up, rate_base, head_gain, out_weight,
    )
    mixed = exchange(
        part, tokens.reshape(2, ROWS, D), mid_gain.reshape(-1, 128), route_ids.T, route_weights.T,
        blend_vector, jnp.swapaxes(expert_gate, 1, 2),
        jnp.swapaxes(expert_up, 1, 2), expert_down, dense_gate.T, dense_up.T, dense_down,
    )
    return (mixed.reshape(2 * ROWS, D // 2), new_state)


def solution(mesh):
    split = Mesh(mesh.devices.reshape(NZ, NY, NX, mesh.shape["tp"]), EP_TP)
    in_specs = (
        P(EP, None),
        P(EP, "tp", None, None),
        P(),
        P(None, "tp"),
        P(None, "tp"),
        P(None, "tp"),
        P(),
        P(None, "tp"),
        P("tp"),
        P(),
        P(None, "tp"),
        P("tp"),
        P("tp"),
        P("tp", None),
        P(),
        P(EP, None),
        P(EP, None),
        P(EP, None, "tp"),
        P(EP, None, "tp"),
        P(EP, "tp", None),
        P(None, EP_TP),
        P(None, EP_TP),
        P(EP_TP, None),
        P(),
    )
    out_specs = (P(EP, "tp"), P(EP, "tp", None, None))
    return jax.shard_map(
        shards, mesh=split, in_specs=in_specs, out_specs=out_specs, check_vma=False
    )
```
